32 devices in a mesh: sp: 16 (over z, x, core), tp: 2 (over y).
Axes of the slice: x: 2, y: 2, z: 4, core: 2. Of those that a mesh axis runs over, the one named last changes fastest.
Arguments:
- value_rows: bfloat16 [16384, 1024], P('sp', 'tp'), may hold values from -6 to 6
- gate_rows: bfloat16 [16384, 1024], P('sp', 'tp'), may hold values from -6 to 6
- conv_taps: bfloat16 [31, 1024], P(None, 'tp'), may hold values from -1 to 1
- norm_gain: float32 [1024], P('tp'), may hold values from 0.1 to 1.9
- point_weight: bfloat16 [1024, 1024], P(None, 'tp'), may hold values from -0.1875 to 0.1875
- out_grad: bfloat16 [16384, 1024], P('sp', 'tp'), may hold values from -6 to 6
Outputs:
- value_grad: bfloat16 [16384, 1024], P('sp', 'tp')
- gate_grad: bfloat16 [16384, 1024], P('sp', 'tp')
- taps_grad: float32 [31, 1024], P(None, 'tp')
- gain_grad: float32 [1024], P('tp')
- weight_grad: float32 [1024, 1024], P('sp', 'tp')
The draws below stay inside these ranges and needn't reach their ends.
All inputs are finite; a program needn't handle non-finite values.
Results may differ from the reference program's by a relative error of at most 0.0051.
Values may be sent and summed in bfloat16 or wider, within the bound.
A program may use at most 128 MiB of HBM per device.

```python
import jax
import jax.numpy as jnp
from jax import lax

C = 1024
GROUP = 64
KW = 31
HALF = 15
TOK_DEV = 1024
TOKENS = 16384


def raised(array, key, source, target, blocks, factor):
    def block_of(dim):
        return (jnp.arange(array.shape[dim]) // (array.shape[dim] // blocks)).reshape((-1,) + (1,) * (array.ndim - 1 - dim))

    near = jax.random.permutation(key, blocks)[block_of(target)]
    second = (block_of(target) + blocks // 2) % blocks
    return jnp.where((block_of(source) == near) | (block_of(source) == second), factor * array, array)


def block_levels(rng, dims, cuts, least, largest):
    def one(position, shards_of):
        draws = jax.random.uniform(jax.random.fold_in(jax.random.fold_in(rng, 6), position), (shards_of,), jnp.float32, least / len(cuts), largest / len(cuts))
        return jnp.repeat(jnp.exp(draws), dims[position] // shards_of).reshape((-1,) + (1,) * (len(dims) - position - 1))

    loudness = one(*cuts[0])
    for cut in cuts[1:]:
        loudness = loudness * one(*cut)
    return loudness


def gaussian(key, shape, deviation, most, pieces=(), held_as=jnp.bfloat16):
    result = jax.random.normal(key, shape, jnp.float32) * deviation
    if len(pieces) > 0:
        result = block_levels(key, shape, pieces, -0.22, 0.18) * result
    return jnp.clip(result, min=-most, max=most).astype(held_as)


def heavy_noise(stream_key, dims, deviation, most, shards, heavy, held_as=jnp.bfloat16):
    drawn = deviation * jax.random.normal(stream_key, dims, jnp.float32)
    if shards:
        drawn = drawn * block_levels(stream_key, dims, shards, -0.22, 0.18)
    return jnp.clip(raised(drawn, jax.random.fold_in(stream_key, 3), *heavy), -most, most).astype(held_as)


def setup_inputs(seed: int = 0) -> dict:
    splits = jax.random.split(jax.random.key(seed), 7)
    return {
        "value_rows": gaussian(splits[0], (TOKENS, C), 1.0, 6.0, ((0, 16), (1, 2))),
        "gate_rows": gaussian(splits[1], (TOKENS, C), 1.0, 6.0, ((0, 16), (1, 2))),
        "conv_taps": gaussian(splits[2], (KW, C), KW ** -0.5, 1.0, ((1, 2),)),
        "norm_gain": jnp.clip(1.0 + 0.18 * jax.random.normal(splits[3], (C,), jnp.float32), 0.1, 1.9),
        "point_weight": gaussian(splits[4], (C, C), C ** -0.5, 0.1875, ((1, 2),)),
        "out_grad": heavy_noise(splits[5], (TOKENS, C), 1.0, 6.0, ((0, 16), (1, 2)), (0, 1, 16, 2.0)),
    }


EPS = 1e-06

def reference(value_rows, gate_rows, conv_taps, norm_gain, point_weight, out_grad):
    total_rows = value_rows.shape[0]
    block_rows = TOK_DEV
    block_count = total_rows // block_rows
    groups = C // GROUP
    gate_sig_all = jax.nn.sigmoid(gate_rows.astype(jnp.float32))
    gated_all = (value_rows.astype(jnp.float32) * gate_sig_all).astype(jnp.bfloat16)
    gated_pad = jnp.pad(gated_all, ((2 * HALF, 2 * HALF), (0, 0)))
    grad_pad = jnp.pad(out_grad, ((HALF, HALF), (0, 0)))
    taps_f = conv_taps.astype(jnp.float32)
    gain_g = norm_gain.astype(jnp.float32).reshape(groups, GROUP)
    extent = block_rows + 2 * HALF

    def one_block(carry, block_index):
        taps_acc, gain_acc, weight_acc = carry
        start = (block_index * block_rows).astype(jnp.int32)
        gated_wide = lax.dynamic_slice_in_dim(gated_pad, start, block_rows + 4 * HALF, 0)
        cotangent = lax.dynamic_slice_in_dim(grad_pad, start, extent, 0)
        value_f = lax.dynamic_slice_in_dim(value_rows, start, block_rows, 0).astype(jnp.float32)
        gate_sig = lax.dynamic_slice_in_dim(gate_sig_all, start, block_rows, 0)
        convolved = jnp.zeros((extent, C), jnp.float32)
        for tap_index in range(KW):
            convolved = convolved + taps_f[tap_index] * gated_wide[tap_index:tap_index + extent].astype(jnp.float32)
        grouped = convolved.reshape(extent, groups, GROUP)
        group_mean = lax.optimization_barrier(jnp.mean(grouped, axis=-1, keepdims=True))
        centred = grouped - group_mean
        inv_std = lax.rsqrt(lax.optimization_barrier(jnp.mean(centred * centred, axis=-1, keepdims=True)) + EPS)
        unit_conv = centred * inv_std
        pre_act = unit_conv * gain_g
        act_sig = jax.nn.sigmoid(pre_act)
        normed = (pre_act * act_sig).astype(jnp.bfloat16).reshape(extent, C)
        normed_grad = jnp.dot(cotangent, point_weight, preferred_element_type=jnp.float32).reshape(extent, groups, GROUP)
        own_grad = cotangent[HALF:HALF + block_rows]
        own_normed = normed[HALF:HALF + block_rows]
        weight_part = lax.dot_general(own_grad, own_normed, (((0,), (0,)), ((), ())), preferred_element_type=jnp.float32)
        act_grad = normed_grad * act_sig * (1.0 + pre_act * (1.0 - act_sig))
        gain_part = lax.optimization_barrier(jnp.sum((act_grad * unit_conv)[HALF:HALF + block_rows], axis=0)).reshape(C)
        hat_grad = act_grad * gain_g
        conv_grad = inv_std * (hat_grad - lax.optimization_barrier(jnp.mean(hat_grad, axis=-1, keepdims=True)) - unit_conv * lax.optimization_barrier(jnp.mean(hat_grad * unit_conv, axis=-1, keepdims=True)))
        conv_grad = conv_grad.reshape(extent, C)
        own_conv = conv_grad[HALF:HALF + block_rows]
        taps_part = jnp.stack([lax.optimization_barrier(jnp.sum(own_conv * gated_wide[HALF + tap_index:HALF + tap_index + block_rows].astype(jnp.float32), axis=0)) for tap_index in range(KW)])
        gated_grad = jnp.zeros((block_rows, C), jnp.float32)
        for tap_index in range(KW):
            lower = 2 * HALF - tap_index
            gated_grad = gated_grad + taps_f[tap_index] * conv_grad[lower:lower + block_rows]
        value_grad = (gated_grad * gate_sig).astype(jnp.bfloat16)
        gate_grad = (gated_grad * value_f * gate_sig * (1.0 - gate_sig)).astype(jnp.bfloat16)
        return ((taps_acc + taps_part, gain_acc + gain_part, weight_acc + weight_part), (value_grad, gate_grad))
    init = (jnp.zeros((KW, C), jnp.float32), jnp.zeros((C,), jnp.float32), jnp.zeros((C, C), jnp.float32))
    sums, blocks = lax.scan(one_block, init, jnp.arange(block_count, dtype=jnp.int32))
    taps_grad, gain_grad, weight_grad = sums
    value_grad = blocks[0].reshape(total_rows, C)
    gate_grad = blocks[1].reshape(total_rows, C)
    return (value_grad, gate_grad, taps_grad, gain_grad, weight_grad)
```

```python
import functools

import jax
import jax.numpy as jnp
from jax import lax
from jax.experimental import pallas as pl
from jax.experimental.pallas import tpu as pltpu
from jax.sharding import PartitionSpec as P

GROUP = 64
EPS = 1e-06
LANE = 128
EDGE = 16
WIDE = 2 * EDGE
SEG = 16
TAU = 8
CHUNK = SEG * TAU
UNIT = 2 * LANE
F32, BF16 = jnp.float32, jnp.bfloat16


def sigmoid(x):
    return 0.5 * jnp.tanh(0.5 * x) + 0.5


def divisor(total, *choices):
    for choice in choices:
        if total % choice == 0:
            return choice
    return total


def group_matrix():
    row = lax.broadcasted_iota(jnp.int32, (2 * LANE, LANE), 0)
    col = lax.broadcasted_iota(jnp.int32, (2 * LANE, LANE), 1)
    same = lax.rem(row, LANE) // GROUP == col // GROUP
    return jnp.where(same, 1.0 / GROUP, 0.0).astype(BF16)


def group_mean(x, matrix):
    high = x.astype(BF16)
    low = (x - high.astype(F32)).astype(BF16)
    return jnp.dot(jnp.concatenate([high, low], axis=1), matrix, preferred_element_type=F32)


def near_mean(x, matrix):
    return jnp.dot(x.astype(BF16), matrix[:LANE], preferred_element_type=F32)


def lanes(c):
    return pl.ds(pl.multiple_of(c * LANE, LANE), LANE)


def loop(lo, hi, body):
    def one(i, _):
        body(i)
        return 0

    lax.fori_loop(lo, hi, one, 0)


def put_gated(gated, c, v, g, dst, n):
    gated[c, pl.ds(dst, n), :] = (v.astype(F32) * sigmoid(g.astype(F32))).astype(BF16).astype(F32)


def spread(src, c, low, high, stride):
    half = SEG // 2
    return jnp.concatenate([src[c, pl.ds(low, half, stride=stride), :],
                            src[c, pl.ds(high, half, stride=stride), :]], axis=0).astype(BF16)


def products(pairs):
    sums = [None] * len(pairs)
    for step in zip(*pairs):
        for a, (x, y) in enumerate(step):
            p = x().astype(F32) * y().astype(F32)
            sums[a] = p if sums[a] is None else sums[a] + p
    return sums


def conv_block(kw, source, tapb, c, taus, reverse, put):
    width = min(4, taus)
    for first in range(0, taus, width):
        pairs = []
        for a in range(width):
            tau = first + a
            pairs.append([
                ((lambda j=(tau + kw - 1 - k if reverse else tau + k): source(j)), (lambda k=k: tapb[c, k]))
                for k in range(kw)])
        for a, total in enumerate(products(pairs)):
            put(first + a, total)


def act_to_conv(ng, at, n, own, unit, inv, gain, dconv, gain_part, matrix):
    for c in range(unit.shape[0]):
        g = gain[:, c * LANE:(c + 1) * LANE]
        u = unit[c, pl.ds(at, n), :]
        p = u * g
        s = sigmoid(p)
        a = ng[:, c * LANE:(c + 1) * LANE] * s * (1.0 + p * (1.0 - s))
        au = a * u
        if own:
            gain_part[:, c * LANE:(c + 1) * LANE] += jnp.sum(au.reshape(n // 8, 8, LANE), axis=0)
        h = a * g
        hu = au * g
        dconv[c, pl.ds(at, n), :] = inv[c, pl.ds(at, n), :] * (
            h - near_mean(h, matrix) - u * near_mean(hu, matrix))


def whole_kernel(n, peers, value_in, gate_in, taps_in, gain_in, weight_in, grad_in,
                 vgrad_out, ggrad_out, taps_out, gain_out, wout,
                 value, gate, weight, grad, taps_raw, gain, vgrad, ggrad, taps, tapb, tacc, lsem, osem,
                 gated, shifted, edges, unit, inv, normed, dconv, dshift, dpack, grow, ngacc,
                 gain_part, wpart, sums,
                 vhalo, ohalo, others, send1, recv1, send2, recv2, send3, recv3,
                 arecv1, asend2, arecv2, atotal, asend3, arecv3,
                 vs, vr, os_, or_, gs, gr, ws, wr, ws3, wr3, as_, ar, as3, ar3):
    rows, chans = value.shape
    tiles = chans // LANE
    kw = taps.shape[1]
    sp, tp = lax.axis_index("sp"), lax.axis_index("tp")
    group = recv3.shape[0] + 1
    half_tiles = tiles // 2
    b0, b1, zz = lax.rem(sp, 2), lax.rem(sp // 2, 2), sp // 4
    has_left, has_right = sp > 0, sp < n - 1
    left, right = lax.rem(sp + n - 1, n), lax.rem(sp + 1, n)
    mate0 = sp + 1 - 2 * b0
    mate1 = sp + 2 - 4 * b1
    chunks = rows // CHUNK
    owned = chans // UNIT
    units = (peers - 1) * owned

    def zmate(d):
        return lax.rem(sp + 4 * d, n)

    def tmate(j):
        return lax.rem(tp + peers - j, peers)

    def remote(src, dst, s, r, to):
        return pltpu.make_async_remote_copy(
            src_ref=src, dst_ref=dst, send_sem=s, recv_sem=r, device_id=to,
            device_id_type=pl.DeviceIdType.MESH)

    barrier = pltpu.get_barrier_semaphore()

    def hello(friend):
        pl.semaphore_signal(barrier, inc=1, device_id=friend, device_id_type=pl.DeviceIdType.MESH)

    friends = [(sp, tmate(j)) for j in range(1, peers)] + [(mate0, tp), (mate1, tp)]
    friends += [(zmate(d), tp) for d in range(1, group)]
    for friend in friends:
        hello(friend)

    @pl.when(has_left)
    def _():
        for j in range(peers):
            hello((left, tmate(j)))

    @pl.when(has_right)
    def _():
        for j in range(peers):
            hello((right, tmate(j)))

    loads = [pltpu.make_async_copy(src, dst, lsem.at[i]) for i, (src, dst) in enumerate(
        ((grad_in, grad), (value_in, value), (gate_in, gate), (taps_in, taps_raw), (gain_in, gain), (weight_in, weight)))]
    for copy in loads:
        copy.start()
    loads[0].wait()
    pl.semaphore_wait(barrier, len(friends) + peers * (has_left.astype(jnp.int32) + has_right.astype(jnp.int32)))

    halos = [[remote(ref.at[pl.ds(start, WIDE)], vhalo.at[side, i], vs.at[side, i], vr.at[side, i], (to, tp))
              for i, ref in enumerate((value_in, gate_in))]
             for side, (start, to) in enumerate(((rows - WIDE, right), (0, left)))]
    ohalos = [[remote(grad.at[pl.ds(start, EDGE)], ohalo.at[side, j], os_.at[side, j], or_.at[side, j], (to, tmate(j)))
               for j in range(peers)]
              for side, (start, to) in enumerate(((rows - EDGE, right), (0, left)))]
    sends = (has_right, has_left)
    arrives = (has_left, has_right)

    def unit_lane(p):
        p = lax.rem(p, owned)
        return pl.multiple_of(jnp.where(2 * tp < peers, owned - 1 - p, p) * UNIT, UNIT)

    def gather(p, r):
        j = p // owned + 1
        at = (pl.ds(pl.multiple_of(r * CHUNK, CHUNK), CHUNK), pl.ds(unit_lane(p), UNIT))
        return remote(grad.at[at], others.at[(j - 1,) + at], gs.at[p, r], gr.at[p, r], (sp, tmate(j)))

    def start_halos(copies):
        for side in range(2):
            @pl.when(sends[side])
            def _(side=side):
                for copy in copies[side]:
                    copy.start()

    def unit_lane_from(p):
        j = p // owned + 1
        sender = lax.rem(tp + j, peers)
        q = lax.rem(p, owned)
        return pl.multiple_of(jnp.where(2 * sender < peers, owned - 1 - q, q) * UNIT, UNIT)

    start_halos(halos)
    for p in range(units):
        for r in range(chunks):
            gather(p, r).start()
        if p == 0:
            start_halos(ohalos)

    matrix = group_matrix()
    loads[3].wait()
    for c in range(tiles):
        taps[c] = taps_raw[:, c * LANE:(c + 1) * LANE].astype(F32)

    def widen(c):
        for k in range(kw):
            tapb[c, k] = jnp.broadcast_to(taps[c, pl.ds(k, 1), :], (SEG, LANE)).astype(BF16)

    loop(0, tiles, widen)
    gain_part[...] = jnp.zeros_like(gain_part)
    tacc[...] = jnp.zeros_like(tacc)
    loads[1].wait()
    loads[2].wait()
    gstep = divisor(rows, 256, 32)

    def own_gated(c):
        def chunk(r):
            at = pl.multiple_of(r * gstep, gstep)
            put_gated(gated, c, value[pl.ds(at, gstep), lanes(c)], gate[pl.ds(at, gstep), lanes(c)],
                      pl.multiple_of(at + WIDE, 8), gstep)

        loop(0, rows // gstep, chunk)

    loop(0, tiles, own_gated)

    def put_halos():
        for side, dst in ((0, 0), (1, rows + WIDE)):
            @pl.when(arrives[side])
            def _(side=side, dst=dst):
                for copy in halos[side]:
                    copy.wait_recv()

                def one(c):
                    put_gated(gated, c, vhalo[side, 0, :, lanes(c)], vhalo[side, 1, :, lanes(c)], dst, WIDE)

                loop(0, tiles, one)

            @pl.when(jnp.logical_not(arrives[side]))
            def _(dst=dst):
                for c in range(tiles):
                    gated[c, pl.ds(dst, WIDE), :] = jnp.zeros((WIDE, LANE), F32)

    def forward(i):
        r = lax.rem(i + 1, chunks)
        base = r * CHUNK

        @pl.when(i == chunks - 2)
        def _():
            put_halos()

        def tile(c):
            for j in range(TAU + kw - 1):
                low = base + (j + WIDE - kw // 2)
                shifted[c, r, j] = spread(gated, c, low, low + TAU * (SEG // 2), TAU)

            def put(tau, total):
                for h in range(2):
                    start = base + (EDGE + tau + h * TAU * (SEG // 2))
                    unit[c, pl.ds(start, SEG // 2, stride=TAU), :] = total[h * (SEG // 2):(h + 1) * (SEG // 2)]

            conv_block(kw, lambda j: shifted[c, r, j], tapb, c, TAU, False, put)

        loop(0, tiles, tile)

    loop(0, chunks, forward)

    def forward_edges(c):
        for j in range(2 + kw - 1):
            edges[j] = spread(gated, c, EDGE - kw // 2 + j, rows + WIDE - kw // 2 + j, 2)

        def put(tau, total):
            for h, start in ((0, tau), (1, rows + EDGE + tau)):
                unit[c, pl.ds(start, SEG // 2, stride=2), :] = total[h * (SEG // 2):(h + 1) * (SEG // 2)]

        conv_block(kw, lambda j: edges[j], tapb, c, 2, False, put)

    loop(0, tiles, forward_edges)
    loads[4].wait()

    def norm_rows(c, at, count):
        x = unit[c, pl.ds(at, count), :]
        centred = x - group_mean(x, matrix)
        rs = lax.rsqrt(near_mean(centred * centred, matrix) + EPS)
        inv[c, pl.ds(at, count), :] = rs
        u = centred * rs
        unit[c, pl.ds(at, count), :] = u
        return u

    nstep = divisor(rows, 256, 32)

    def norm(c):
        def chunk(r):
            at = pl.multiple_of(r * nstep, nstep)
            p = norm_rows(c, pl.multiple_of(at + EDGE, 8), nstep) * gain[:, lanes(c)]
            normed[pl.ds(at, nstep), lanes(c)] = (p * sigmoid(p)).astype(BF16)

        loop(0, rows // nstep, chunk)
        norm_rows(c, 0, EDGE)
        norm_rows(c, rows + EDGE, EDGE)

    loop(0, tiles, norm)

    def owner(j):
        return lax.rem(tp + j, peers)

    per = wpart.shape[1]
    span = UNIT // per

    def unit_of(j, p):
        lane = unit_lane_from((j - 1) * owned + p) if j else pl.multiple_of(p * UNIT, UNIT)
        return lane, (owner(j) * chans + lane) // per

    def weight_part(j, p, first, count, add):
        lane, base = unit_of(j, p)
        at = (pl.ds(first, count), pl.ds(lane, UNIT))
        lhs = others[(j - 1,) + at] if j else grad[at]
        out = lax.dot_general(lhs, normed[pl.ds(first, count), :], (((0,), (0,)), ((), ())), preferred_element_type=F32)
        out = out.reshape(span, per, chans)
        wpart[pl.ds(base, span)] = wpart[pl.ds(base, span)] + out if add else out

    pairs, quads, far = span // 2, span // 4, span // 4

    def half1(j, p):
        at = pl.ds(unit_of(j, p)[1] // 2, pairs)
        k = j * owned + p
        return remote(send1.at[at], recv1.at[at], ws.at[0, k], wr.at[0, k], (mate0, tp))

    def half2(j, p):
        at = pl.ds(unit_of(j, p)[1] // 4, quads)
        k = j * owned + p
        return remote(send2.at[at], recv2.at[at], ws.at[1, k], wr.at[1, k], (mate1, tp))

    def start1(j, p):
        first = unit_of(j, p)[1] // 2

        def cast(i):
            send1[first + i] = wpart[2 * (first + i) + 1 - b0].astype(BF16)

        loop(0, pairs, cast)
        half1(j, p).start()

    def start2(j, p):
        first = unit_of(j, p)[1] // 4
        half1(j, p).wait_recv()

        def cast(i):
            other, mine = 2 * (first + i) + 1 - b1, 2 * (first + i) + b1
            send2[first + i] = (wpart[2 * other + b0] + recv1[other].astype(F32)).astype(BF16)
            wpart[2 * mine + b0] = wpart[2 * mine + b0] + recv1[mine].astype(F32)

        loop(0, quads, cast)
        half2(j, p).start()

    def total2(z):
        return wpart[4 * z + 2 * b1 + b0] + recv2[z].astype(F32)

    def final_copy(slot):
        return remote(send3.at[slot], recv3.at[slot], ws3.at[slot], wr3.at[slot],
                      (lax.rem(sp + 4 * (slot + 1), n), tp))

    def start3(j, p):
        half2(j, p).wait_recv()
        first = unit_of(j, p)[1] // 4

        def one(i):
            z = first + i
            d = lax.rem(z + group - zz, group)

            @pl.when(d != 0)
            def _():
                send3[d - 1] = total2(z).astype(BF16)
                final_copy(d - 1).start()

        loop(0, far, one)

    def weight_rows(j, lane):
        return pl.ds(pl.multiple_of(owner(j) * chans + lane, UNIT), UNIT)

    def partial_ng(r):
        at = pl.ds(pl.multiple_of(r * nstep, nstep), nstep)
        total = jnp.dot(grad[at, :], weight[pl.ds(pl.multiple_of(owner(0) * chans, UNIT), chans), :],
                        preferred_element_type=F32)
        for p in range(units - 1):
            lane = unit_lane_from(p)
            j = p // owned + 1
            total += jnp.dot(others[j - 1, at, pl.ds(lane, UNIT)], weight[weight_rows(j, lane), :],
                             preferred_element_type=F32)
        ngacc[at, :] = total

    last_lane = unit_lane_from(units - 1)

    def middle(r):
        gather(units - 1, r).wait_recv()
        at = pl.ds(pl.multiple_of(r * CHUNK, CHUNK), CHUNK)
        ng = ngacc[at, :] + jnp.dot(others[peers - 2, at, pl.ds(last_lane, UNIT)], weight[weight_rows(peers - 1, last_lane), :],
                                    preferred_element_type=F32)
        act_to_conv(ng, pl.multiple_of(r * CHUNK + EDGE, 8), CHUNK, True, unit, inv, gain, dconv, gain_part, matrix)

    def taps_chunk(r):
        def tile(c):
            for tau in range(TAU):
                low = r * CHUNK + (EDGE + tau)
                dpack[c, tau] = spread(dconv, c, low, low + TAU * (SEG // 2), TAU)
            for k0 in range(0, kw, 4):
                ks = range(k0, min(k0 + 4, kw))
                pairs_ = [[((lambda j=tau + k: shifted[c, r, j]), (lambda tau=tau: dpack[c, tau])) for tau in range(TAU)]
                          for k in ks]
                for k, total in zip(ks, products(pairs_)):
                    tacc[c, k] += total[:SEG // 2] + total[SEG // 2:]

        loop(0, tiles, tile)

    def finalize(r):
        middle(r)
        taps_chunk(r)

    def fold_taps(c):
        for k in range(kw):
            sums[c, pl.ds(k, 1), :] = jnp.sum(tacc[c, k], axis=0, keepdims=True)
        sums[c, pl.ds(kw, 1), :] = jnp.sum(gain_part[:, lanes(c)], axis=0, keepdims=True)

    def edge_conv():
        for side, at in ((0, 0), (1, rows + EDGE)):
            @pl.when(arrives[side])
            def _(side=side, at=at):
                for copy in ohalos[side]:
                    copy.wait_recv()
                ng = sum(jnp.dot(ohalo[side, j], weight[pl.ds(pl.multiple_of(owner(j) * chans, UNIT), chans), :],
                                 preferred_element_type=F32) for j in range(peers))
                act_to_conv(ng, at, EDGE, False, unit, inv, gain, dconv, gain_part, matrix)

            @pl.when(jnp.logical_not(arrives[side]))
            def _(at=at):
                for c in range(tiles):
                    dconv[c, pl.ds(at, EDGE), :] = jnp.zeros((EDGE, LANE), F32)

    def backward(r):
        def tile(c):
            base = r * CHUNK
            for j in range(TAU + kw - 1):
                low = base + (EDGE - kw // 2 + j)
                dshift[j] = spread(dconv, c, low, low + TAU * (SEG // 2), TAU)

            def put(tau, total):
                for h in range(2):
                    grow[c, pl.ds(tau + h * TAU * (SEG // 2), SEG // 2, stride=TAU), :] = (
                        total[h * (SEG // 2):(h + 1) * (SEG // 2)])

            conv_block(kw, lambda j: dshift[j], tapb, c, TAU, True, put)
            at = pl.ds(pl.multiple_of(base, CHUNK), CHUNK)
            s = sigmoid(gate[at, lanes(c)].astype(F32))
            v = value[at, lanes(c)].astype(F32)
            out = grow[c] * s
            vgrad[at, lanes(c)] = out.astype(BF16)
            ggrad[at, lanes(c)] = (out * v * (1.0 - s)).astype(BF16)

        loop(0, tiles, tile)
        for copy in out_copies(r):
            copy.start()

    def out_copies(r):
        at = pl.ds(pl.multiple_of(r * CHUNK, CHUNK), CHUNK)
        return (pltpu.make_async_copy(vgrad.at[at], vgrad_out.at[at], osem.at[0, r]),
                pltpu.make_async_copy(ggrad.at[at], ggrad_out.at[at], osem.at[1, r]))

    for p in range(owned):
        weight_part(0, p, 0, rows, False)
        start1(0, p)
    for p in range(owned):
        start2(0, p)
    loads[5].wait()
    for p in range(units - 1):
        for r in range(chunks):
            gather(p, r).wait_recv()
        weight_part(p // owned + 1, p % owned, 0, rows, False)
        start1(p // owned + 1, p % owned)
    loop(0, rows // nstep, partial_ng)
    for p in range(owned):
        start3(0, p)
    edge_conv()
    for p in range(units - 1):
        start2(p // owned + 1, p % owned)
    lj, lp = peers - 1, owned - 1
    loop(0, chunks - 2, finalize)
    for p in range(units - 1):
        start3(p // owned + 1, p % owned)
    weight_part(lj, lp, 0, rows - 2 * CHUNK, False)
    finalize(chunks - 2)
    middle(chunks - 1)
    weight_part(lj, lp, rows - 2 * CHUNK, 2 * CHUNK, True)
    start1(lj, lp)
    taps_chunk(chunks - 1)
    loop(0, tiles, fold_taps)

    acopy1 = remote(sums.at[pl.ds((1 - b0) * half_tiles, half_tiles)], arecv1, as_.at[0], ar.at[0], (mate0, tp))
    acopy1.start()
    start2(lj, lp)
    acopy1.wait_recv()
    mine = (sums[pl.ds(b0 * half_tiles, half_tiles)] + arecv1[...]).astype(BF16)
    asend2[...] = mine
    acopy2 = remote(asend2, arecv2, as_.at[1], ar.at[1], (mate1, tp))
    acopy2.start()
    backward(0)
    backward(1)
    acopy2.wait_recv()
    asend3[...] = (asend2[...].astype(F32) + arecv2[...].astype(F32)).astype(BF16)
    acopies3 = []
    for d in range(1, group):
        copy = remote(asend3, arecv3.at[zz], as3.at[d - 1], ar3.at[d - 1], (zmate(d), tp))
        copy.start()
        acopies3.append(copy)
    loop(2, 4, backward)
    start3(lj, lp)
    loop(4, chunks, backward)
    arecv3[zz] = asend3[...]
    for d in range(1, group):
        peer = lax.rem(zz + group - d, group)
        remote(asend3, arecv3.at[peer], as3.at[d - 1], ar3.at[d - 1], (zmate(d), tp)).wait_recv()
    total = arecv3[0].astype(F32)
    for z in range(1, group):
        total += arecv3[z].astype(F32)
    atotal[b0] = total
    acopy4 = remote(atotal.at[b0], atotal.at[b0], as_.at[2], ar.at[2], (mate0, tp))
    acopy4.start()
    final = total2(zz)
    for d in range(1, group):
        final_copy(d - 1).wait_recv()
        final += recv3[d - 1].astype(F32)
    wout[...] = final
    remote(atotal.at[1 - b0], atotal.at[1 - b0], as_.at[2], ar.at[2], (mate0, tp)).wait_recv()
    for c in range(tiles):
        tot = atotal[c // half_tiles, c % half_tiles]
        taps_out[:, c * LANE:(c + 1) * LANE] = tot[:kw]
        gain_out[:, c * LANE:(c + 1) * LANE] = tot[kw:]
    for side in range(2):
        @pl.when(sends[side])
        def _(side=side):
            for copy in halos[side] + ohalos[side]:
                copy.wait_send()
    for copy in [acopy1, acopy2, acopy4] + acopies3:
        copy.wait_send()
    for p in range(units):
        for r in range(chunks):
            gather(p, r).wait_send()
    for j in range(peers):
        for p in range(owned):
            half1(j, p).wait_send()
            half2(j, p).wait_send()
    for d in range(1, group):
        final_copy(d - 1).wait_send()

    def drain(r):
        for copy in out_copies(r):
            copy.wait()

    loop(0, chunks, drain)


def finish_kernel(parts, *refs):
    count = len(parts)
    sources, targets, held = refs[:count], refs[count:2 * count], refs[2 * count:3 * count]
    isem, osem = refs[3 * count:]
    incoming, outgoing = [], []
    slot = 0
    for src, dst, buf, pieces in zip(sources, targets, held, parts):
        size = src.shape[0] // pieces
        for p in range(pieces):
            at = pl.ds(p * size, size)
            incoming.append(pltpu.make_async_copy(src.at[at], buf.at[at], isem.at[slot]))
            outgoing.append(pltpu.make_async_copy(buf.at[at], dst.at[at], osem.at[slot]))
            slot += 1
    for copy in incoming:
        copy.start()
    for copy, after in zip(incoming, outgoing):
        copy.wait()
        after.start()
    for copy in outgoing:
        copy.wait()


def finish(*arrays):
    parts = [4 if a.shape[0] % 128 == 0 else 1 for a in arrays]
    sems = pltpu.SemaphoreType.DMA((sum(parts),))
    return pl.pallas_call(
        functools.partial(finish_kernel, parts),
        out_shape=[jax.ShapeDtypeStruct(a.shape, a.dtype) for a in arrays],
        in_specs=[pl.BlockSpec(memory_space=pl.ANY)] * len(arrays),
        out_specs=[pl.BlockSpec(memory_space=pl.ANY)] * len(arrays),
        scratch_shapes=[pltpu.VMEM(a.shape, a.dtype) for a in arrays] + [sems, sems],
        compiler_params=pltpu.CompilerParams(vmem_limit_bytes=60 * 1024 * 1024),
    )(*arrays)


def per_device(value, gate, conv_taps, norm_gain, point_weight, out_grad):
    rows, chans = value.shape
    kw = conv_taps.shape[0]
    tiles = chans // LANE
    n, peers = lax.axis_size("sp"), lax.axis_size("tp")
    extent = rows + WIDE
    full = point_weight.shape[0]
    per = full // n
    group = n // 4
    chunks = rows // CHUNK
    owned = chans // UNIT
    units = (peers - 1) * owned
    gain = norm_gain.reshape(1, chans)
    args = (value, gate, conv_taps, gain, point_weight, out_grad)
    half = (tiles // 2, kw + 1, LANE)
    vmem, dma = pltpu.VMEM, pltpu.SemaphoreType.DMA
    block = (SEG, LANE)
    outs = [((rows, chans), BF16), ((rows, chans), BF16), ((kw, chans), F32), ((1, chans), F32), ((per, chans), F32)]
    vgrad, ggrad, taps_grad, gain_grad, wgrad = pl.pallas_call(
        functools.partial(whole_kernel, n, peers),
        out_shape=[jax.ShapeDtypeStruct(s, d) for s, d in outs],
        in_specs=[pl.BlockSpec(memory_space=pl.ANY)] * 6,
        out_specs=[pl.BlockSpec(memory_space=m) for m in (pl.ANY, pl.ANY, vmem, vmem, vmem)],
        scratch_shapes=[
            vmem((rows, chans), BF16), vmem((rows, chans), BF16), vmem((full, chans), BF16), vmem((rows, chans), BF16),
            vmem((kw, chans), BF16), vmem((1, chans), F32),
            vmem((rows, chans), BF16), vmem((rows, chans), BF16),
            vmem((tiles, kw, LANE), F32),
            vmem((tiles, kw) + block, BF16),
            vmem((tiles, kw, 8, LANE), F32),
            dma((6,)), dma((2, chunks)),
            vmem((tiles, rows + 4 * EDGE, LANE), F32),
            vmem((tiles, chunks, TAU + kw - 1) + block, BF16),
            vmem((kw + 1,) + block, BF16),
            vmem((tiles, extent, LANE), F32),
            vmem((tiles, extent, LANE), F32),
            vmem((rows, chans), BF16),
            vmem((tiles, extent, LANE), F32),
            vmem((TAU + kw - 1,) + block, BF16),
            vmem((tiles, TAU) + block, BF16),
            vmem((tiles, CHUNK, LANE), F32),
            vmem((rows, chans), F32),
            vmem((8, chans), F32),
            vmem((n, per, chans), F32),
            vmem((tiles, kw + 1, LANE), F32),
            vmem((2, 2, WIDE, chans), BF16),
            vmem((2, peers, EDGE, chans), BF16),
            vmem((peers - 1, rows, chans), BF16),
            vmem((n // 2, per, chans), BF16),
            vmem((n // 2, per, chans), BF16),
            vmem((n // 4, per, chans), BF16),
            vmem((n // 4, per, chans), BF16),
            vmem((group - 1, per, chans), BF16),
            vmem((group - 1, per, chans), BF16),
            vmem(half, F32),
            vmem(half, BF16),
            vmem(half, BF16),
            vmem((2,) + half, F32),
            vmem(half, BF16),
            vmem((group,) + half, BF16),
            dma((2, 2)), dma((2, 2)), dma((2, peers)), dma((2, peers)),
            dma((units, chunks)), dma((units, chunks)),
            dma((2, peers * owned)), dma((2, peers * owned)), dma((group - 1,)), dma((group - 1,)),
            dma((3,)), dma((3,)), dma((group - 1,)), dma((group - 1,)),
        ],
        compiler_params=pltpu.CompilerParams(
            collective_id=0, has_side_effects=True, vmem_limit_bytes=60 * 1024 * 1024),
    )(*args)
    vgrad, ggrad, taps_grad, gain_grad, wgrad = finish(vgrad, ggrad, taps_grad, gain_grad, wgrad)
    return vgrad, ggrad, taps_grad, gain_grad.reshape(chans), wgrad


def solution(mesh):
    return jax.shard_map(
        per_device,
        mesh=mesh,
        in_specs=(P("sp", "tp"), P("sp", "tp"), P(None, "tp"), P("tp"), P(None, "tp"), P("sp", "tp")),
        out_specs=(P("sp", "tp"), P("sp", "tp"), P(None, "tp"), P("tp"), P("sp", "tp")),
        check_vma=False,
    )
```

```python
import functools

import jax
import jax.numpy as jnp
from jax import lax
from jax.experimental import pallas as pl
from jax.experimental.pallas import tpu as pltpu
from jax.sharding import PartitionSpec as P

GROUP = 64
EPS = 1e-06
LANE = 128
EDGE = 16
WIDE = 2 * EDGE
SEG = 16
TAU = 8
CHUNK = SEG * TAU
UNIT = 2 * LANE
F32, BF16 = jnp.float32, jnp.bfloat16


def sigmoid(x):
    return 0.5 * jnp.tanh(0.5 * x) + 0.5


def divisor(total, *choices):
    for choice in choices:
        if total % choice == 0:
            return choice
    return total


def group_matrix():
    row = lax.broadcasted_iota(jnp.int32, (2 * LANE, LANE), 0)
    col = lax.broadcasted_iota(jnp.int32, (2 * LANE, LANE), 1)
    same = lax.rem(row, LANE) // GROUP == col // GROUP
    return jnp.where(same, 1.0 / GROUP, 0.0).astype(BF16)


def group_mean(x, matrix):
    high = x.astype(BF16)
    low = (x - high.astype(F32)).astype(BF16)
    return jnp.dot(jnp.concatenate([high, low], axis=1), matrix, preferred_element_type=F32)


def near_mean(x, matrix):
    return jnp.dot(x.astype(BF16), matrix[:LANE], preferred_element_type=F32)


def lanes(c):
    return pl.ds(pl.multiple_of(c * LANE, LANE), LANE)


def loop(lo, hi, body):
    def one(i, _):
        body(i)
        return 0

    lax.fori_loop(lo, hi, one, 0)


def put_gated(gated, c, v, g, dst, n):
    gated[c, pl.ds(dst, n), :] = (v.astype(F32) * sigmoid(g.astype(F32))).astype(BF16).astype(F32)


def spread(src, c, low, high, stride):
    half = SEG // 2
    return jnp.concatenate([src[c, pl.ds(low, half, stride=stride), :],
                            src[c, pl.ds(high, half, stride=stride), :]], axis=0).astype(BF16)


def products(pairs):
    sums = [None] * len(pairs)
    for step in zip(*pairs):
        for a, (x, y) in enumerate(step):
            p = x().astype(F32) * y().astype(F32)
            sums[a] = p if sums[a] is None else sums[a] + p
    return sums


def conv_block(kw, source, tapb, c, taus, reverse, put):
    width = min(4, taus)
    for first in range(0, taus, width):
        pairs = []
        for a in range(width):
            tau = first + a
            pairs.append([
                ((lambda j=(tau + kw - 1 - k if reverse else tau + k): source(j)), (lambda k=k: tapb[c, k]))
                for k in range(kw)])
        for a, total in enumerate(products(pairs)):
            put(first + a, total)


def act_to_conv(ng, at, n, own, unit, inv, gain, dconv, gain_part, matrix):
    for c in range(unit.shape[0]):
        g = gain[:, c * LANE:(c + 1) * LANE]
        u = unit[c, pl.ds(at, n), :]
        p = u * g
        s = sigmoid(p)
        a = ng[:, c * LANE:(c + 1) * LANE] * s * (1.0 + p * (1.0 - s))
        au = a * u
        if own:
            gain_part[:, c * LANE:(c + 1) * LANE] += jnp.sum(au.reshape(n // 8, 8, LANE), axis=0)
        h = a * g
        hu = au * g
        dconv[c, pl.ds(at, n), :] = inv[c, pl.ds(at, n), :] * (
            h - near_mean(h, matrix) - u * near_mean(hu, matrix))


def whole_kernel(n, peers, value_in, gate_in, taps_in, gain_in, weight_in, grad_in,
                 vgrad, ggrad, taps_out, gain_out, wout,
                 value, gate, weight, grad, taps_raw, gain, taps, tapb, tacc, lsem,
                 gated, shifted, edges, unit, inv, normed, dconv, dshift, dpack, grow, ngacc,
                 gain_part, wpart, sums,
                 vhalo, ohalo, others, send1, recv1, send2, recv2, send3, recv3,
                 asend, arecv, atotal, zsend, zrecv,
                 vs, vr, os_, or_, gs, gr, ws, wr, ws3, wr3, as_, ar, as3, ar3):
    rows, chans = value.shape
    tiles = chans // LANE
    kw = taps.shape[1]
    sp, tp = lax.axis_index("sp"), lax.axis_index("tp")
    group = recv3.shape[0] + 1
    b0, b1, zz = lax.rem(sp, 2), lax.rem(sp // 2, 2), sp // 4
    has_left, has_right = sp > 0, sp < n - 1
    left, right = lax.rem(sp + n - 1, n), lax.rem(sp + 1, n)
    mate0 = sp + 1 - 2 * b0
    mate1 = sp + 2 - 4 * b1
    chunks = rows // CHUNK
    owned = chans // UNIT
    units = (peers - 1) * owned

    quarter = lax.rem(sp, 4)

    def plane(d):
        return sp - quarter + lax.rem(quarter + d, 4)

    def zmate(d):
        return lax.rem(sp + 4 * d, n)

    def tmate(j):
        return lax.rem(tp + peers - j, peers)

    def remote(src, dst, s, r, to):
        return pltpu.make_async_remote_copy(
            src_ref=src, dst_ref=dst, send_sem=s, recv_sem=r, device_id=to,
            device_id_type=pl.DeviceIdType.MESH)

    barrier = pltpu.get_barrier_semaphore()

    def hello(friend):
        pl.semaphore_signal(barrier, inc=1, device_id=friend, device_id_type=pl.DeviceIdType.MESH)

    friends = [(sp, tmate(j)) for j in range(1, peers)] + [(plane(d), tp) for d in range(1, 4)]
    friends += [(zmate(d), tp) for d in range(1, group)]
    for friend in friends:
        hello(friend)

    @pl.when(has_left)
    def _():
        for j in range(peers):
            hello((left, tmate(j)))

    @pl.when(has_right)
    def _():
        for j in range(peers):
            hello((right, tmate(j)))

    loads = [pltpu.make_async_copy(src, dst, lsem.at[i]) for i, (src, dst) in enumerate(
        ((grad_in, grad), (value_in, value), (gate_in, gate), (taps_in, taps_raw), (gain_in, gain), (weight_in, weight)))]
    loads = loads[1:3] + loads[:1] + loads[3:]
    for copy in loads:
        copy.start()
    pl.semaphore_wait(barrier, len(friends) + peers * (has_left.astype(jnp.int32) + has_right.astype(jnp.int32)))

    halos = [[remote(ref.at[pl.ds(start, WIDE)], vhalo.at[side, i], vs.at[side, i], vr.at[side, i], (to, tp))
              for i, ref in enumerate((value_in, gate_in))]
             for side, (start, to) in enumerate(((rows - WIDE, right), (0, left)))]
    ohalos = [[remote(grad_in.at[pl.ds(start, EDGE)], ohalo.at[side, j], os_.at[side, j], or_.at[side, j], (to, tmate(j)))
               for j in range(peers)]
              for side, (start, to) in enumerate(((rows - EDGE, right), (0, left)))]
    sends = (has_right, has_left)
    arrives = (has_left, has_right)

    def unit_lane(p):
        p = lax.rem(p, owned)
        return pl.multiple_of(jnp.where(2 * tp < peers, p, owned - 1 - p) * UNIT, UNIT)

    def gather(p, r):
        j = p // owned + 1
        at = (pl.ds(pl.multiple_of(r * CHUNK, CHUNK), CHUNK), pl.ds(unit_lane(p), UNIT))
        return remote(grad_in.at[at], others.at[(j - 1,) + at], gs.at[p, r], gr.at[p, r], (sp, tmate(j)))

    def start_halos(copies):
        for side in range(2):
            @pl.when(sends[side])
            def _(side=side):
                for copy in copies[side]:
                    copy.start()

    def unit_lane_from(p):
        j = p // owned + 1
        sender = lax.rem(tp + j, peers)
        q = lax.rem(p, owned)
        return pl.multiple_of(jnp.where(2 * sender < peers, q, owned - 1 - q) * UNIT, UNIT)

    start_halos(halos)
    for p in range(units):
        for r in range(chunks):
            gather(p, r).start()
    start_halos(ohalos)

    matrix = group_matrix()
    loads[3].wait()
    for c in range(tiles):
        taps[c] = taps_raw[:, c * LANE:(c + 1) * LANE].astype(F32)

    def widen(c):
        for k in range(kw):
            tapb[c, k] = jnp.broadcast_to(taps[c, pl.ds(k, 1), :], (SEG, LANE)).astype(BF16)

    loop(0, tiles, widen)
    gain_part[...] = jnp.zeros_like(gain_part)
    tacc[...] = jnp.zeros_like(tacc)
    loads[0].wait()
    loads[1].wait()
    gstep = divisor(rows, 256, 32)

    def own_gated(c):
        def chunk(r):
            at = pl.multiple_of(r * gstep, gstep)
            put_gated(gated, c, value[pl.ds(at, gstep), lanes(c)], gate[pl.ds(at, gstep), lanes(c)],
                      pl.multiple_of(at + WIDE, 8), gstep)

        loop(0, rows // gstep, chunk)

    loop(0, tiles, own_gated)

    def put_halos():
        for side, dst in ((0, 0), (1, rows + WIDE)):
            @pl.when(arrives[side])
            def _(side=side, dst=dst):
                for copy in halos[side]:
                    copy.wait_recv()

                def one(c):
                    put_gated(gated, c, vhalo[side, 0, :, lanes(c)], vhalo[side, 1, :, lanes(c)], dst, WIDE)

                loop(0, tiles, one)

            @pl.when(jnp.logical_not(arrives[side]))
            def _(dst=dst):
                for c in range(tiles):
                    gated[c, pl.ds(dst, WIDE), :] = jnp.zeros((WIDE, LANE), F32)

    def forward(i):
        r = lax.rem(i + 1, chunks)
        base = r * CHUNK

        @pl.when(i == chunks - 2)
        def _():
            put_halos()

        def tile(c):
            for j in range(TAU + kw - 1):
                low = base + (j + WIDE - kw // 2)
                shifted[c, r, j] = spread(gated, c, low, low + TAU * (SEG // 2), TAU)

            def put(tau, total):
                for h in range(2):
                    start = base + (EDGE + tau + h * TAU * (SEG // 2))
                    unit[c, pl.ds(start, SEG // 2, stride=TAU), :] = total[h * (SEG // 2):(h + 1) * (SEG // 2)]

            conv_block(kw, lambda j: shifted[c, r, j], tapb, c, TAU, False, put)

        loop(0, tiles, tile)

    loop(0, chunks, forward)

    def forward_edges(c):
        for j in range(2 + kw - 1):
            edges[j] = spread(gated, c, EDGE - kw // 2 + j, rows + WIDE - kw // 2 + j, 2)

        def put(tau, total):
            for h, start in ((0, tau), (1, rows + EDGE + tau)):
                unit[c, pl.ds(start, SEG // 2, stride=2), :] = total[h * (SEG // 2):(h + 1) * (SEG // 2)]

        conv_block(kw, lambda j: edges[j], tapb, c, 2, False, put)

    loop(0, tiles, forward_edges)
    loads[4].wait()

    def norm_rows(at, count):
        xs = [unit[c, pl.ds(at, count), :] for c in range(tiles)]
        centred = [x - group_mean(x, matrix) for x in xs]
        out = []
        for c in range(tiles):
            rs = lax.rsqrt(near_mean(centred[c] * centred[c], matrix) + EPS)
            inv[c, pl.ds(at, count), :] = rs
            u = centred[c] * rs
            unit[c, pl.ds(at, count), :] = u
            out.append(u)
        return out

    def norm(r):
        at = pl.multiple_of(r * CHUNK, CHUNK)
        for c, u in enumerate(norm_rows(pl.multiple_of(at + EDGE, 8), CHUNK)):
            p = u * gain[:, c * LANE:(c + 1) * LANE]
            normed[pl.ds(at, CHUNK), c * LANE:(c + 1) * LANE] = (p * sigmoid(p)).astype(BF16)

    loop(0, chunks, norm)
    norm_rows(0, EDGE)
    norm_rows(rows + EDGE, EDGE)
    nstep = divisor(rows, 256, 32)

    def owner(j):
        return lax.rem(tp + j, peers)

    per = wpart.shape[1]
    span = UNIT // per

    def unit_of(j, p):
        lane = unit_lane_from((j - 1) * owned + p) if j else pl.multiple_of(p * UNIT, UNIT)
        return lane, (owner(j) * chans + lane) // per

    def weight_part(j, p, first, count, add):
        lane, base = unit_of(j, p)
        at = (pl.ds(first, count), pl.ds(lane, UNIT))
        lhs = others[(j - 1,) + at] if j else grad[at]
        out = lax.dot_general(lhs, normed[pl.ds(first, count), :], (((0,), (0,)), ((), ())), preferred_element_type=F32)
        out = out.reshape(span, per, chans)
        wpart[pl.ds(base, span)] = wpart[pl.ds(base, span)] + out if add else out

    pairs, quads, far = span // 2, span // 4, span // 4

    def half1(j, p):
        at = pl.ds(unit_of(j, p)[1] // 2, pairs)
        k = j * owned + p
        return remote(send1.at[at], recv1.at[at], ws.at[0, k], wr.at[0, k], (mate0, tp))

    def half2(j, p):
        at = pl.ds(unit_of(j, p)[1] // 4, quads)
        k = j * owned + p
        return remote(send2.at[at], recv2.at[at], ws.at[1, k], wr.at[1, k], (mate1, tp))

    def start1(j, p):
        first = unit_of(j, p)[1] // 2

        def cast(i):
            send1[first + i] = wpart[2 * (first + i) + 1 - b0].astype(BF16)

        loop(0, pairs, cast)
        half1(j, p).start()

    def start2(j, p):
        first = unit_of(j, p)[1] // 4
        half1(j, p).wait_recv()

        def cast(i):
            other, mine = 2 * (first + i) + 1 - b1, 2 * (first + i) + b1
            send2[first + i] = (wpart[2 * other + b0] + recv1[other].astype(F32)).astype(BF16)
            wpart[2 * mine + b0] = wpart[2 * mine + b0] + recv1[mine].astype(F32)

        loop(0, quads, cast)
        half2(j, p).start()

    def total2(z):
        return wpart[4 * z + 2 * b1 + b0] + recv2[z].astype(F32)

    def final_copy(slot):
        return remote(send3.at[slot], recv3.at[slot], ws3.at[slot], wr3.at[slot],
                      (lax.rem(sp + 4 * (slot + 1), n), tp))

    def start3(j, p):
        half2(j, p).wait_recv()
        first = unit_of(j, p)[1] // 4

        def one(i):
            z = first + i
            d = lax.rem(z + group - zz, group)

            @pl.when(d != 0)
            def _():
                send3[d - 1] = total2(z).astype(BF16)
                final_copy(d - 1).start()

        loop(0, far, one)

    def weight_rows(j, lane):
        return pl.ds(pl.multiple_of(owner(j) * chans + lane, UNIT), UNIT)

    def own_ng(r):
        at = pl.ds(pl.multiple_of(r * nstep, nstep), nstep)
        ngacc[at, :] = jnp.dot(grad[at, :], weight[pl.ds(pl.multiple_of(owner(0) * chans, UNIT), chans), :],
                               preferred_element_type=F32)

    def unit_ng(p):
        def add(r):
            at = pl.ds(pl.multiple_of(r * nstep, nstep), nstep)
            lane = unit_lane_from(p)
            j = p // owned + 1
            ngacc[at, :] += jnp.dot(others[j - 1, at, pl.ds(lane, UNIT)], weight[weight_rows(j, lane), :],
                                    preferred_element_type=F32)

        loop(0, rows // nstep, add)

    last_lane = unit_lane_from(units - 1)

    def middle(r):
        at = pl.ds(pl.multiple_of(r * CHUNK, CHUNK), CHUNK)
        ng = ngacc[at, :] + jnp.dot(others[peers - 2, at, pl.ds(last_lane, UNIT)], weight[weight_rows(peers - 1, last_lane), :],
                                    preferred_element_type=F32)
        act_to_conv(ng, pl.multiple_of(r * CHUNK + EDGE, 8), CHUNK, True, unit, inv, gain, dconv, gain_part, matrix)

    def taps_chunk(r):
        def tile(c):
            for tau in range(TAU):
                low = r * CHUNK + (EDGE + tau)
                dpack[c, tau] = spread(dconv, c, low, low + TAU * (SEG // 2), TAU)
            for k0 in range(0, kw, 4):
                ks = range(k0, min(k0 + 4, kw))
                pairs_ = [[((lambda j=tau + k: shifted[c, r, j]), (lambda tau=tau: dpack[c, tau])) for tau in range(TAU)]
                          for k in ks]
                for k, total in zip(ks, products(pairs_)):
                    tacc[c, k] += total[:SEG // 2] + total[SEG // 2:]

        loop(0, tiles, tile)

    def finalize(r):
        gather(units - 1, r).wait_recv()
        middle(r)
        taps_chunk(r)

    def fold_taps(c):
        for k in range(kw):
            sums[c, pl.ds(k, 1), :] = jnp.sum(tacc[c, k], axis=0, keepdims=True)
        sums[c, pl.ds(kw, 1), :] = jnp.sum(gain_part[:, lanes(c)], axis=0, keepdims=True)

    def edge_conv():
        for side, at in ((0, 0), (1, rows + EDGE)):
            @pl.when(arrives[side])
            def _(side=side, at=at):
                for copy in ohalos[side]:
                    copy.wait_recv()
                ng = sum(jnp.dot(ohalo[side, j], weight[pl.ds(pl.multiple_of(owner(j) * chans, UNIT), chans), :],
                                 preferred_element_type=F32) for j in range(peers))
                act_to_conv(ng, at, EDGE, False, unit, inv, gain, dconv, gain_part, matrix)

            @pl.when(jnp.logical_not(arrives[side]))
            def _(at=at):
                for c in range(tiles):
                    dconv[c, pl.ds(at, EDGE), :] = jnp.zeros((EDGE, LANE), F32)

    def backward(r):
        def tile(c):
            base = r * CHUNK
            for j in range(TAU + kw - 1):
                low = base + (EDGE - kw // 2 + j)
                dshift[j] = spread(dconv, c, low, low + TAU * (SEG // 2), TAU)

            def put(tau, total):
                for h in range(2):
                    grow[c, pl.ds(tau + h * TAU * (SEG // 2), SEG // 2, stride=TAU), :] = (
                        total[h * (SEG // 2):(h + 1) * (SEG // 2)])

            conv_block(kw, lambda j: dshift[j], tapb, c, TAU, True, put)
            at = pl.ds(pl.multiple_of(base, CHUNK), CHUNK)
            s = sigmoid(gate[at, lanes(c)].astype(F32))
            v = value[at, lanes(c)].astype(F32)
            out = grow[c] * s
            vgrad[at, lanes(c)] = out.astype(BF16)
            ggrad[at, lanes(c)] = (out * v * (1.0 - s)).astype(BF16)

        loop(0, tiles, tile)

    part = (kw + 1) // 4

    def slot(d):
        return lax.rem(quarter + d, 4)

    def gather_sums(d):
        return remote(asend.at[slot(d)], arecv.at[d - 1], as_.at[0, d - 1], ar.at[0, d - 1], (plane(d), tp))

    def share(d):
        return remote(atotal.at[quarter], atotal.at[quarter], as_.at[1, d - 1], ar.at[1, d - 1], (plane(d), tp))

    def shared_from(d):
        return remote(atotal.at[slot(4 - d)], atotal.at[slot(4 - d)], as_.at[1, d - 1], ar.at[1, d - 1], (plane(d), tp))

    loads[2].wait()
    for p in range(owned):
        weight_part(0, p, 0, rows, False)
        start1(0, p)
    loads[5].wait()
    loop(0, rows // nstep, own_ng)
    for p in range(owned):
        start2(0, p)
    for p in range(units - 1):
        for r in range(chunks):
            gather(p, r).wait_recv()
        weight_part(p // owned + 1, p % owned, 0, rows, False)
        start1(p // owned + 1, p % owned)
        unit_ng(p)
    for p in range(owned):
        start3(0, p)
    for p in range(units - 1):
        start2(p // owned + 1, p % owned)
    lj, lp = peers - 1, owned - 1
    loop(0, 3, finalize)
    for p in range(units - 1):
        start3(p // owned + 1, p % owned)
    loop(3, chunks - 2, finalize)
    weight_part(lj, lp, 0, rows - 2 * CHUNK, False)
    finalize(chunks - 2)
    gather(units - 1, chunks - 1).wait_recv()
    weight_part(lj, lp, rows - 2 * CHUNK, 2 * CHUNK, True)
    start1(lj, lp)
    middle(chunks - 1)
    taps_chunk(chunks - 1)
    loop(0, tiles, fold_taps)
    for q in range(4):
        asend[q] = sums[:, q * part:(q + 1) * part, :].astype(BF16)
    for d in range(1, 4):
        gather_sums(d).start()
    start2(lj, lp)
    loop(1, 5, backward)
    for d in range(1, 4):
        gather_sums(d).wait_recv()
    mine = sums[:, pl.ds(pl.multiple_of(quarter * part, part), part), :]
    for d in range(3):
        mine += arecv[d].astype(F32)
    zsend[...] = mine.astype(BF16)
    acopies3 = []
    for d in range(1, group):
        copy = remote(zsend, zrecv.at[zz], as3.at[d - 1], ar3.at[d - 1], (zmate(d), tp))
        copy.start()
        acopies3.append(copy)
    edge_conv()
    backward(0)
    backward(chunks - 1)
    start3(lj, lp)
    loop(5, chunks - 1, backward)
    zrecv[zz] = zsend[...]
    for d in range(1, group):
        peer = lax.rem(zz + group - d, group)
        remote(zsend, zrecv.at[peer], as3.at[d - 1], ar3.at[d - 1], (zmate(d), tp)).wait_recv()
    total = zrecv[0].astype(F32)
    for z in range(1, group):
        total += zrecv[z].astype(F32)
    atotal[quarter] = total
    for d in range(1, 4):
        share(d).start()
    final = total2(zz)
    for d in range(1, group):
        final_copy(d - 1).wait_recv()
        final += recv3[d - 1].astype(F32)
    wout[...] = final
    for d in range(1, 4):
        shared_from(d).wait_recv()
    for c in range(tiles):
        tot = jnp.concatenate([atotal[q, c] for q in range(4)], axis=0)
        taps_out[:, c * LANE:(c + 1) * LANE] = tot[:kw]
        gain_out[:, c * LANE:(c + 1) * LANE] = tot[kw:]
    for side in range(2):
        @pl.when(sends[side])
        def _(side=side):
            for copy in halos[side] + ohalos[side]:
                copy.wait_send()
    for copy in acopies3 + [gather_sums(d) for d in range(1, 4)] + [share(d) for d in range(1, 4)]:
        copy.wait_send()
    for p in range(units):
        for r in range(chunks):
            gather(p, r).wait_send()
    for j in range(peers):
        for p in range(owned):
            half1(j, p).wait_send()
            half2(j, p).wait_send()
    for d in range(1, group):
        final_copy(d - 1).wait_send()


def finish_kernel(parts, *refs):
    count = len(parts)
    sources, targets, osem = refs[:count], refs[count:2 * count], refs[2 * count]
    outgoing = []
    for src, dst, pieces in zip(sources, targets, parts):
        size = src.shape[0] // pieces
        for p in range(pieces):
            at = pl.ds(p * size, size)
            outgoing.append(pltpu.make_async_copy(src.at[at], dst.at[at], osem.at[len(outgoing)]))
    for copy in outgoing:
        copy.start()
    for copy in outgoing:
        copy.wait()


def finish(*arrays):
    parts = [4 if a.shape[0] % 128 == 0 else 1 for a in arrays]
    return pl.pallas_call(
        functools.partial(finish_kernel, parts),
        out_shape=[jax.ShapeDtypeStruct(a.shape, a.dtype) for a in arrays],
        in_specs=[pl.BlockSpec(memory_space=pltpu.VMEM)] * len(arrays),
        out_specs=[pl.BlockSpec(memory_space=pl.ANY)] * len(arrays),
        scratch_shapes=[pltpu.SemaphoreType.DMA((sum(parts),))],
    )(*[pltpu.with_memory_space_constraint(a, pltpu.VMEM) for a in arrays])


def per_device(value, gate, conv_taps, norm_gain, point_weight, out_grad):
    rows, chans = value.shape
    kw = conv_taps.shape[0]
    tiles = chans // LANE
    n, peers = lax.axis_size("sp"), lax.axis_size("tp")
    extent = rows + WIDE
    full = point_weight.shape[0]
    per = full // n
    group = n // 4
    chunks = rows // CHUNK
    owned = chans // UNIT
    units = (peers - 1) * owned
    gain = norm_gain.reshape(1, chans)
    args = (value, gate, conv_taps, gain, point_weight, out_grad)
    piece = (tiles, (kw + 1) // 4, LANE)
    vmem, dma = pltpu.VMEM, pltpu.SemaphoreType.DMA
    block = (SEG, LANE)
    outs = [((rows, chans), BF16), ((rows, chans), BF16), ((kw, chans), F32), ((1, chans), F32), ((per, chans), F32)]
    vgrad, ggrad, taps_grad, gain_grad, wgrad = pl.pallas_call(
        functools.partial(whole_kernel, n, peers),
        out_shape=[vmem(s, d) for s, d in outs],
        in_specs=[pl.BlockSpec(memory_space=pl.ANY)] * 6,
        out_specs=[pl.BlockSpec(memory_space=vmem)] * len(outs),
        scratch_shapes=[
            vmem((rows, chans), BF16), vmem((rows, chans), BF16), vmem((full, chans), BF16), vmem((rows, chans), BF16),
            vmem((kw, chans), BF16), vmem((1, chans), F32),
            vmem((tiles, kw, LANE), F32),
            vmem((tiles, kw) + block, BF16),
            vmem((tiles, kw, 8, LANE), F32),
            dma((6,)),
            vmem((tiles, rows + 4 * EDGE, LANE), F32),
            vmem((tiles, chunks, TAU + kw - 1) + block, BF16),
            vmem((kw + 1,) + block, BF16),
            vmem((tiles, extent, LANE), F32),
            vmem((tiles, extent, LANE), F32),
            vmem((rows, chans), BF16),
            vmem((tiles, extent, LANE), F32),
            vmem((TAU + kw - 1,) + block, BF16),
            vmem((tiles, TAU) + block, BF16),
            vmem((tiles, CHUNK, LANE), F32),
            vmem((rows, chans), F32),
            vmem((8, chans), F32),
            vmem((n, per, chans), F32),
            vmem((tiles, kw + 1, LANE), F32),
            vmem((2, 2, WIDE, chans), BF16),
            vmem((2, peers, EDGE, chans), BF16),
            vmem((peers - 1, rows, chans), BF16),
            vmem((n // 2, per, chans), BF16),
            vmem((n // 2, per, chans), BF16),
            vmem((n // 4, per, chans), BF16),
            vmem((n // 4, per, chans), BF16),
            vmem((group - 1, per, chans), BF16),
            vmem((group - 1, per, chans), BF16),
            vmem((4,) + piece, BF16),
            vmem((3,) + piece, BF16),
            vmem((4,) + piece, F32),
            vmem(piece, BF16),
            vmem((group,) + piece, BF16),
            dma((2, 2)), dma((2, 2)), dma((2, peers)), dma((2, peers)),
            dma((units, chunks)), dma((units, chunks)),
            dma((2, peers * owned)), dma((2, peers * owned)), dma((group - 1,)), dma((group - 1,)),
            dma((2, 3)), dma((2, 3)), dma((group - 1,)), dma((group - 1,)),
        ],
        compiler_params=pltpu.CompilerParams(
            collective_id=0, has_side_effects=True, vmem_limit_bytes=52 * 1024 * 1024),
    )(*args)
    vgrad, ggrad, taps_grad, gain_grad, wgrad = finish(vgrad, ggrad, taps_grad, gain_grad, wgrad)
    return vgrad, ggrad, taps_grad, gain_grad.reshape(chans), wgrad


def solution(mesh):
    return jax.shard_map(
        per_device,
        mesh=mesh,
        in_specs=(P("sp", "tp"), P("sp", "tp"), P(None, "tp"), P("tp"), P(None, "tp"), P("sp", "tp")),
        out_specs=(P("sp", "tp"), P("sp", "tp"), P(None, "tp"), P("tp"), P("sp", "tp")),
        check_vma=False,
    )
```

```python
import functools

import jax
import jax.numpy as jnp
from jax import lax
from jax.experimental import pallas as pl
from jax.experimental.pallas import tpu as pltpu
from jax.sharding import PartitionSpec as P

GROUP = 64
EPS = 1e-06
LANE = 128
EDGE = 16
WIDE = 2 * EDGE
SEG = 16
TAU = 8
CHUNK = SEG * TAU
UNIT = 2 * LANE
F32, BF16 = jnp.float32, jnp.bfloat16


def sigmoid(x):
    return 0.5 * jnp.tanh(0.5 * x) + 0.5


def divisor(total, *choices):
    for choice in choices:
        if total % choice == 0:
            return choice
    return total


def group_matrix(stacked):
    row = lax.broadcasted_iota(jnp.int32, (2 * LANE, 2 * LANE), 0)
    col = lax.broadcasted_iota(jnp.int32, (2 * LANE, 2 * LANE), 1)
    if stacked:
        row, col = lax.rem(row, LANE), lax.rem(col, LANE)
    return jnp.where(row // GROUP == col // GROUP, 1.0 / GROUP, 0.0).astype(BF16)


def group_mean(x, stacked):
    high = x.astype(BF16)
    low = (x - high.astype(F32)).astype(BF16)
    return jnp.dot(jnp.concatenate([high, low], axis=1), stacked[:, :LANE], preferred_element_type=F32)


def near_means(x, y, apart):
    both = jnp.dot(jnp.concatenate([x.astype(BF16), y.astype(BF16)], axis=1), apart, preferred_element_type=F32)
    return both[:, :LANE], both[:, LANE:]


def lanes(c):
    return pl.ds(pl.multiple_of(c * LANE, LANE), LANE)


def loop(lo, hi, body):
    def one(i, _):
        body(i)
        return 0

    lax.fori_loop(lo, hi, one, 0)


def put_gated(gated, c, v, g, dst, n):
    gated[c, pl.ds(dst, n), :] = (v.astype(F32) * sigmoid(g.astype(F32))).astype(BF16).astype(F32)


def spread(src, c, low, high, stride):
    half = SEG // 2
    return jnp.concatenate([src[c, pl.ds(low, half, stride=stride), :],
                            src[c, pl.ds(high, half, stride=stride), :]], axis=0).astype(BF16)


def products(pairs):
    sums = [None] * len(pairs)
    for step in zip(*pairs):
        for a, (x, y) in enumerate(step):
            p = x().astype(F32) * y().astype(F32)
            sums[a] = p if sums[a] is None else sums[a] + p
    return sums


def conv_block(kw, source, tapb, c, taus, reverse, put):
    width = min(4, taus)
    for first in range(0, taus, width):
        pairs = []
        for a in range(width):
            tau = first + a
            pairs.append([
                ((lambda j=(tau + kw - 1 - k if reverse else tau + k): source(j)), (lambda k=k: tapb[c, k]))
                for k in range(kw)])
        for a, total in enumerate(products(pairs)):
            put(first + a, total)


def act_to_conv(ng, at, n, own, unit, inv, slope, gain, dconv, gain_part, apart):
    for c in range(unit.shape[0]):
        g = gain[:, c * LANE:(c + 1) * LANE]
        u = unit[c, pl.ds(at, n), :]
        a = ng[:, c * LANE:(c + 1) * LANE] * slope[c, pl.ds(at, n), :]
        au = a * u
        if own:
            gain_part[:, c * LANE:(c + 1) * LANE] += jnp.sum(au.reshape(n // 8, 8, LANE), axis=0)
        h = a * g
        first, second = near_means(h, au * g, apart)
        dconv[c, pl.ds(at, n), :] = inv[c, pl.ds(at, n), :] * (h - first - u * second)


def whole_kernel(n, peers, value_in, gate_in, taps_in, gain_in, weight_in, grad_in,
                 vgrad, ggrad, taps_out, gain_out, wout,
                 value, gate, weight, grad, taps_raw, gain, taps, tapb, tacc,
                 gated, shifted, edges, unit, inv, slope, normed, dconv, dshift, dpack, grow, ngacc,
                 gain_part, wpart, sums,
                 vhalo, ohalo, others, send1, recv1, send2, recv2, send3, recv3,
                 asend, arecv, atotal, zsend, zrecv,
                 lsem, vs, vr, os_, or_, gs, gr, ws, wr, ws3, wr3, as_, ar, as3, ar3):
    rows, chans = value.shape
    tiles = chans // LANE
    kw = taps.shape[1]
    sp, tp = lax.axis_index("sp"), lax.axis_index("tp")
    group = recv3.shape[0] + 1
    b0, b1, zz = lax.rem(sp, 2), lax.rem(sp // 2, 2), sp // 4
    has_left, has_right = sp > 0, sp < n - 1
    left, right = lax.rem(sp + n - 1, n), lax.rem(sp + 1, n)
    mate0 = sp + 1 - 2 * b0
    mate1 = sp + 2 - 4 * b1
    chunks = rows // CHUNK
    owned = chans // UNIT
    units = (peers - 1) * owned

    quarter = lax.rem(sp, 4)

    def plane(d):
        return sp - quarter + lax.rem(quarter + d, 4)

    def zmate(d):
        return lax.rem(sp + 4 * d, n)

    def tmate(j):
        return lax.rem(tp + peers - j, peers)

    def remote(src, dst, s, r, to):
        return pltpu.make_async_remote_copy(
            src_ref=src, dst_ref=dst, send_sem=s, recv_sem=r, device_id=to,
            device_id_type=pl.DeviceIdType.MESH)

    barrier = pltpu.get_barrier_semaphore()

    def hello(friend):
        pl.semaphore_signal(barrier, inc=1, device_id=friend, device_id_type=pl.DeviceIdType.MESH)

    friends = [(sp, tmate(j)) for j in range(1, peers)] + [(plane(d), tp) for d in range(1, 4)]
    friends += [(zmate(d), tp) for d in range(1, group)]
    for friend in friends:
        hello(friend)

    @pl.when(has_left)
    def _():
        for j in range(peers):
            hello((left, tmate(j)))

    @pl.when(has_right)
    def _():
        for j in range(peers):
            hello((right, tmate(j)))

    loads = [pltpu.make_async_copy(src, dst, lsem.at[i]) for i, (src, dst) in enumerate(
        ((grad_in, grad), (value_in, value), (gate_in, gate), (taps_in, taps_raw), (gain_in, gain), (weight_in, weight)))]
    loads = loads[1:3] + loads[:1] + loads[3:]
    for copy in loads:
        copy.start()
    pl.semaphore_wait(barrier, len(friends) + peers * (has_left.astype(jnp.int32) + has_right.astype(jnp.int32)))

    halos = [[remote(ref.at[pl.ds(start, WIDE)], vhalo.at[side, i], vs.at[side, i], vr.at[side, i], (to, tp))
              for i, ref in enumerate((value_in, gate_in))]
             for side, (start, to) in enumerate(((rows - WIDE, right), (0, left)))]
    ohalos = [[remote(grad_in.at[pl.ds(start, EDGE)], ohalo.at[side, j], os_.at[side, j], or_.at[side, j], (to, tmate(j)))
               for j in range(peers)]
              for side, (start, to) in enumerate(((rows - EDGE, right), (0, left)))]
    sends = (has_right, has_left)
    arrives = (has_left, has_right)

    def unit_lane(p):
        p = lax.rem(p, owned)
        return pl.multiple_of(jnp.where(2 * tp < peers, p, owned - 1 - p) * UNIT, UNIT)

    def gather(p, r):
        j = p // owned + 1
        at = (pl.ds(pl.multiple_of(r * CHUNK, CHUNK), CHUNK), pl.ds(unit_lane(p), UNIT))
        return remote(grad_in.at[at], others.at[(j - 1,) + at], gs.at[p, r], gr.at[p, r], (sp, tmate(j)))

    def start_halos(copies):
        for side in range(2):
            @pl.when(sends[side])
            def _(side=side):
                for copy in copies[side]:
                    copy.start()

    def unit_lane_from(p):
        j = p // owned + 1
        sender = lax.rem(tp + j, peers)
        q = lax.rem(p, owned)
        return pl.multiple_of(jnp.where(2 * sender < peers, q, owned - 1 - q) * UNIT, UNIT)

    start_halos(halos)
    for p in range(units):
        for r in range(chunks):
            gather(p, r).start()

    stacked, apart = group_matrix(True), group_matrix(False)
    loads[3].wait()
    for c in range(tiles):
        taps[c] = taps_raw[:, c * LANE:(c + 1) * LANE].astype(F32)

    def widen(c):
        for k in range(kw):
            tapb[c, k] = jnp.broadcast_to(taps[c, pl.ds(k, 1), :], (SEG, LANE)).astype(BF16)

    loop(0, tiles, widen)
    gain_part[...] = jnp.zeros_like(gain_part)
    tacc[...] = jnp.zeros_like(tacc)
    loads[0].wait()
    loads[1].wait()
    gstep = divisor(rows, 256, 32)

    def own_gated(c):
        def chunk(r):
            at = pl.multiple_of(r * gstep, gstep)
            put_gated(gated, c, value[pl.ds(at, gstep), lanes(c)], gate[pl.ds(at, gstep), lanes(c)],
                      pl.multiple_of(at + WIDE, 8), gstep)

        loop(0, rows // gstep, chunk)

    loop(0, tiles, own_gated)

    def put_halos():
        for side, dst in ((0, 0), (1, rows + WIDE)):
            @pl.when(arrives[side])
            def _(side=side, dst=dst):
                for copy in halos[side]:
                    copy.wait_recv()

                def one(c):
                    put_gated(gated, c, vhalo[side, 0, :, lanes(c)], vhalo[side, 1, :, lanes(c)], dst, WIDE)

                loop(0, tiles, one)

            @pl.when(jnp.logical_not(arrives[side]))
            def _(dst=dst):
                for c in range(tiles):
                    gated[c, pl.ds(dst, WIDE), :] = jnp.zeros((WIDE, LANE), F32)

    def forward(i):
        r = lax.rem(i + 1, chunks)
        base = r * CHUNK

        @pl.when(i == chunks - 2)
        def _():
            put_halos()

        def tile(c):
            for j in range(TAU + kw - 1):
                low = base + (j + WIDE - kw // 2)
                shifted[c, r, j] = spread(gated, c, low, low + TAU * (SEG // 2), TAU)

            def put(tau, total):
                for h in range(2):
                    start = base + (EDGE + tau + h * TAU * (SEG // 2))
                    unit[c, pl.ds(start, SEG // 2, stride=TAU), :] = total[h * (SEG // 2):(h + 1) * (SEG // 2)]

            conv_block(kw, lambda j: shifted[c, r, j], tapb, c, TAU, False, put)

        loop(0, tiles, tile)

    loop(0, chunks, forward)

    def forward_edges(c):
        for j in range(2 + kw - 1):
            edges[j] = spread(gated, c, EDGE - kw // 2 + j, rows + WIDE - kw // 2 + j, 2)

        def put(tau, total):
            for h, start in ((0, tau), (1, rows + EDGE + tau)):
                unit[c, pl.ds(start, SEG // 2, stride=2), :] = total[h * (SEG // 2):(h + 1) * (SEG // 2)]

        conv_block(kw, lambda j: edges[j], tapb, c, 2, False, put)

    loop(0, tiles, forward_edges)
    loads[4].wait()

    def norm_rows(at, count, own):
        xs = [unit[c, pl.ds(at, count), :] for c in range(tiles)]
        centred = [x - group_mean(x, stacked) for x in xs]
        for c in range(0, tiles, 2):
            spreads = near_means(centred[c] * centred[c], centred[c + 1] * centred[c + 1], apart)
            for e, var in zip((c, c + 1), spreads):
                rs = lax.rsqrt(var + EPS)
                inv[e, pl.ds(at, count), :] = rs
                u = centred[e] * rs
                unit[e, pl.ds(at, count), :] = u
                p = u * gain[:, e * LANE:(e + 1) * LANE]
                s = sigmoid(p)
                slope[e, pl.ds(at, count), :] = s * (1.0 + p * (1.0 - s))
                if own is not None:
                    normed[pl.ds(own, count), e * LANE:(e + 1) * LANE] = (p * s).astype(BF16)

    def norm(r):
        at = pl.multiple_of(r * CHUNK, CHUNK)
        norm_rows(pl.multiple_of(at + EDGE, 8), CHUNK, at)

    loop(0, chunks, norm)
    norm_rows(0, EDGE, None)
    norm_rows(rows + EDGE, EDGE, None)
    nstep = divisor(rows, 256, 32)

    def owner(j):
        return lax.rem(tp + j, peers)

    per = wpart.shape[1]
    span = UNIT // per

    def unit_of(j, p):
        lane = unit_lane_from((j - 1) * owned + p) if j else pl.multiple_of(p * UNIT, UNIT)
        return lane, (owner(j) * chans + lane) // per

    def weight_part(j, p, first, count, add):
        lane, base = unit_of(j, p)
        at = (pl.ds(first, count), pl.ds(lane, UNIT))
        lhs = others[(j - 1,) + at] if j else grad[at]
        out = lax.dot_general(lhs, normed[pl.ds(first, count), :], (((0,), (0,)), ((), ())), preferred_element_type=F32)
        out = out.reshape(span, per, chans)
        wpart[pl.ds(base, span)] = wpart[pl.ds(base, span)] + out if add else out

    pairs, quads, far = span // 2, span // 4, span // 4

    def half1(j, p):
        at = pl.ds(unit_of(j, p)[1] // 2, pairs)
        k = j * owned + p
        return remote(send1.at[at], recv1.at[at], ws.at[0, k], wr.at[0, k], (mate0, tp))

    half = chans // 2

    def cols(h):
        return pl.ds(h * half, half)

    def half2(j, p, h):
        at = (pl.ds(unit_of(j, p)[1] // 4, quads), slice(None), cols(h))
        k = j * owned + p
        return remote(send2.at[at], recv2.at[at], ws.at[1 + h, k], wr.at[1 + h, k], (mate1, tp))

    def start1(j, p):
        first = unit_of(j, p)[1] // 2

        def cast(i):
            send1[first + i] = wpart[2 * (first + i) + 1 - b0].astype(BF16)

        loop(0, pairs, cast)
        half1(j, p).start()

    def start2(j, p):
        first = unit_of(j, p)[1] // 4
        half1(j, p).wait_recv()
        for h in range(2):
            def cast(i, h=h):
                other = 2 * (first + i) + 1 - b1
                send2[first + i, :, cols(h)] = (
                    wpart[2 * other + b0, :, cols(h)] + recv1[other, :, cols(h)].astype(F32)).astype(BF16)

            loop(0, quads, cast)
            half2(j, p, h).start()

        def keep(i):
            mine = 2 * (first + i) + b1
            wpart[2 * mine + b0] = wpart[2 * mine + b0] + recv1[mine].astype(F32)

        loop(0, quads, keep)

    def total2(z, h):
        return wpart[4 * z + 2 * b1 + b0, :, cols(h)] + recv2[z, :, cols(h)].astype(F32)

    def final_copy(slot, h):
        at = (slot, slice(None), cols(h))
        return remote(send3.at[at], recv3.at[at], ws3.at[h, slot], wr3.at[h, slot],
                      (lax.rem(sp + 4 * (slot + 1), n), tp))

    def start3(j, p, h):
        half2(j, p, h).wait_recv()
        first = unit_of(j, p)[1] // 4

        def one(i):
            z = first + i
            d = lax.rem(z + group - zz, group)

            @pl.when(d != 0)
            def _():
                send3[d - 1, :, cols(h)] = total2(z, h).astype(BF16)
                final_copy(d - 1, h).start()

        loop(0, far, one)

    def weight_rows(j, lane):
        return pl.ds(pl.multiple_of(owner(j) * chans + lane, UNIT), UNIT)

    def own_ng(r):
        at = pl.ds(pl.multiple_of(r * nstep, nstep), nstep)
        ngacc[at, :] = jnp.dot(grad[at, :], weight[pl.ds(pl.multiple_of(owner(0) * chans, UNIT), chans), :],
                               preferred_element_type=F32)

    def unit_ng(p):
        def add(r):
            at = pl.ds(pl.multiple_of(r * nstep, nstep), nstep)
            lane = unit_lane_from(p)
            j = p // owned + 1
            ngacc[at, :] += jnp.dot(others[j - 1, at, pl.ds(lane, UNIT)], weight[weight_rows(j, lane), :],
                                    preferred_element_type=F32)

        loop(0, rows // nstep, add)

    def middle(r):
        at = pl.ds(pl.multiple_of(r * CHUNK, CHUNK), CHUNK)
        ng = ngacc[at, :] + jnp.dot(others[peers - 2, at, :], weight[pl.ds(pl.multiple_of(owner(peers - 1) * chans, UNIT), chans), :],
                                    preferred_element_type=F32)
        act_to_conv(ng, pl.multiple_of(r * CHUNK + EDGE, 8), CHUNK, True, unit, inv, slope, gain, dconv, gain_part, apart)

    def taps_chunks(*rs):
        def tile(c):
            for i, r in enumerate(rs):
                for tau in range(TAU):
                    low = r * CHUNK + (EDGE + tau)
                    dpack[c, i * TAU + tau] = spread(dconv, c, low, low + TAU * (SEG // 2), TAU)
            for k0 in range(0, kw, 4):
                ks = range(k0, min(k0 + 4, kw))
                pairs_ = [[((lambda r=r, j=tau + k: shifted[c, r, j]), (lambda i=i, tau=tau: dpack[c, i * TAU + tau]))
                           for i, r in enumerate(rs) for tau in range(TAU)] for k in ks]
                for k, total in zip(ks, products(pairs_)):
                    tacc[c, k] += total[:SEG // 2] + total[SEG // 2:]

        loop(0, tiles, tile)

    def finalize(r):
        gather(units - 1, r).wait_recv()
        middle(r)

    def finalize_two(i):
        finalize(2 * i)
        finalize(2 * i + 1)
        taps_chunks(2 * i, 2 * i + 1)

    def fold_taps(c):
        for k in range(kw):
            sums[c, pl.ds(k, 1), :] = jnp.sum(tacc[c, k], axis=0, keepdims=True)
        sums[c, pl.ds(kw, 1), :] = jnp.sum(gain_part[:, lanes(c)], axis=0, keepdims=True)

    def edge_conv():
        for side, at in ((0, 0), (1, rows + EDGE)):
            @pl.when(arrives[side])
            def _(side=side, at=at):
                for copy in ohalos[side]:
                    copy.wait_recv()
                ng = sum(jnp.dot(ohalo[side, j], weight[pl.ds(pl.multiple_of(owner(j) * chans, UNIT), chans), :],
                                 preferred_element_type=F32) for j in range(peers))
                act_to_conv(ng, at, EDGE, False, unit, inv, slope, gain, dconv, gain_part, apart)

            @pl.when(jnp.logical_not(arrives[side]))
            def _(at=at):
                for c in range(tiles):
                    dconv[c, pl.ds(at, EDGE), :] = jnp.zeros((EDGE, LANE), F32)

    def backward(r):
        def tile(c):
            base = r * CHUNK
            for j in range(TAU + kw - 1):
                low = base + (EDGE - kw // 2 + j)
                dshift[j] = spread(dconv, c, low, low + TAU * (SEG // 2), TAU)

            def put(tau, total):
                for h in range(2):
                    grow[c, pl.ds(tau + h * TAU * (SEG // 2), SEG // 2, stride=TAU), :] = (
                        total[h * (SEG // 2):(h + 1) * (SEG // 2)])

            conv_block(kw, lambda j: dshift[j], tapb, c, TAU, True, put)
            at = pl.ds(pl.multiple_of(base, CHUNK), CHUNK)
            s = sigmoid(gate[at, lanes(c)].astype(F32))
            v = value[at, lanes(c)].astype(F32)
            out = grow[c] * s
            vgrad[at, lanes(c)] = out.astype(BF16)
            ggrad[at, lanes(c)] = (out * v * (1.0 - s)).astype(BF16)

        loop(0, tiles, tile)

    part = (kw + 1) // 4

    def slot(d):
        return lax.rem(quarter + d, 4)

    def gather_sums(d):
        return remote(asend.at[slot(d)], arecv.at[d - 1], as_.at[0, d - 1], ar.at[0, d - 1], (plane(d), tp))

    def share(d):
        return remote(atotal.at[quarter], atotal.at[quarter], as_.at[1, d - 1], ar.at[1, d - 1], (plane(d), tp))

    def shared_from(d):
        return remote(atotal.at[slot(4 - d)], atotal.at[slot(4 - d)], as_.at[1, d - 1], ar.at[1, d - 1], (plane(d), tp))

    loads[2].wait()
    for p in range(owned):
        weight_part(0, p, 0, rows, False)
        start1(0, p)
    loads[5].wait()
    loop(0, rows // nstep, own_ng)
    for p in range(owned):
        start2(0, p)
    for p in range(units - 1):
        for r in range(chunks):
            gather(p, r).wait_recv()
        weight_part(p // owned + 1, p % owned, 0, rows, False)
        start1(p // owned + 1, p % owned)
        if p < units - owned:
            unit_ng(p)
    for p in range(owned):
        for h in range(2):
            start3(0, p, h)
    for p in range(units - 1):
        start2(p // owned + 1, p % owned)
    lj, lp = peers - 1, owned - 1
    loop(0, 2, finalize_two)
    for p in range(units - 1):
        for h in range(2):
            start3(p // owned + 1, p % owned, h)
    loop(2, chunks // 2 - 1, finalize_two)
    weight_part(lj, lp, 0, rows - 2 * CHUNK, False)
    finalize(chunks - 2)
    taps_chunks(chunks - 2)
    gather(units - 1, chunks - 1).wait_recv()
    start_halos(ohalos)
    weight_part(lj, lp, rows - 2 * CHUNK, 2 * CHUNK, True)
    start1(lj, lp)
    middle(chunks - 1)
    taps_chunks(chunks - 1)
    loop(0, tiles, fold_taps)
    for q in range(4):
        asend[q] = sums[:, q * part:(q + 1) * part, :].astype(BF16)
    for d in range(1, 4):
        gather_sums(d).start()
    start2(lj, lp)
    loop(1, 5, backward)
    for d in range(1, 4):
        gather_sums(d).wait_recv()
    mine = sums[:, pl.ds(pl.multiple_of(quarter * part, part), part), :]
    for d in range(3):
        mine += arecv[d].astype(F32)
    zsend[...] = mine.astype(BF16)
    acopies3 = []
    for d in range(1, group):
        copy = remote(zsend, zrecv.at[zz], as3.at[d - 1], ar3.at[d - 1], (zmate(d), tp))
        copy.start()
        acopies3.append(copy)
    loop(5, chunks - 1, backward)
    start3(lj, lp, 0)
    edge_conv()
    start3(lj, lp, 1)
    loop(0, 2, lambda i: backward(i * (chunks - 1)))
    zrecv[zz] = zsend[...]
    for d in range(1, group):
        peer = lax.rem(zz + group - d, group)
        remote(zsend, zrecv.at[peer], as3.at[d - 1], ar3.at[d - 1], (zmate(d), tp)).wait_recv()
    total = zrecv[0].astype(F32)
    for z in range(1, group):
        total += zrecv[z].astype(F32)
    atotal[quarter] = total
    for d in range(1, 4):
        share(d).start()
    for h in range(2):
        final = total2(zz, h)
        for d in range(1, group):
            final_copy(d - 1, h).wait_recv()
            final += recv3[d - 1, :, cols(h)].astype(F32)
        wout[:, cols(h)] = final
    for d in range(1, 4):
        shared_from(d).wait_recv()
    for c in range(tiles):
        tot = jnp.concatenate([atotal[q, c] for q in range(4)], axis=0)
        taps_out[:, c * LANE:(c + 1) * LANE] = tot[:kw]
        gain_out[:, c * LANE:(c + 1) * LANE] = tot[kw:]
    for side in range(2):
        @pl.when(sends[side])
        def _(side=side):
            for copy in halos[side] + ohalos[side]:
                copy.wait_send()
    for copy in acopies3 + [gather_sums(d) for d in range(1, 4)] + [share(d) for d in range(1, 4)]:
        copy.wait_send()
    for p in range(units):
        for r in range(chunks):
            gather(p, r).wait_send()
    for j in range(peers):
        for p in range(owned):
            half1(j, p).wait_send()
            for h in range(2):
                half2(j, p, h).wait_send()
    for d in range(1, group):
        for h in range(2):
            final_copy(d - 1, h).wait_send()


def finish_kernel(parts, *refs):
    count = len(parts)
    sources, targets = refs[:count], refs[count:]

    def move(osem):
        outgoing = []
        for src, dst, pieces in zip(sources, targets, parts):
            size = src.shape[0] // pieces
            for p in range(pieces):
                at = pl.ds(p * size, size)
                outgoing.append(pltpu.make_async_copy(src.at[at], dst.at[at], osem.at[len(outgoing)]))
        for copy in outgoing:
            copy.start()
        for copy in outgoing:
            copy.wait()

    pl.run_scoped(move, pltpu.SemaphoreType.DMA((sum(parts),)))


def finish(*arrays):
    parts = [4 if a.shape[0] % 128 == 0 else 1 for a in arrays]
    return pl.pallas_call(
        functools.partial(finish_kernel, parts),
        out_shape=[jax.ShapeDtypeStruct(a.shape, a.dtype) for a in arrays],
        in_specs=[pl.BlockSpec(memory_space=pltpu.VMEM)] * len(arrays),
        out_specs=[pl.BlockSpec(memory_space=pl.ANY)] * len(arrays),
    )(*[pltpu.with_memory_space_constraint(a, pltpu.VMEM) for a in arrays])


def per_device(value, gate, conv_taps, norm_gain, point_weight, out_grad):
    rows, chans = value.shape
    kw = conv_taps.shape[0]
    tiles = chans // LANE
    n, peers = lax.axis_size("sp"), lax.axis_size("tp")
    extent = rows + WIDE
    full = point_weight.shape[0]
    per = full // n
    group = n // 4
    chunks = rows // CHUNK
    owned = chans // UNIT
    units = (peers - 1) * owned
    gain = norm_gain.reshape(1, chans)
    args = (value, gate, conv_taps, gain, point_weight, out_grad)
    piece = (tiles, (kw + 1) // 4, LANE)
    vmem, dma = pltpu.VMEM, pltpu.SemaphoreType.DMA
    block = (SEG, LANE)
    outs = [((rows, chans), BF16), ((rows, chans), BF16), ((kw, chans), F32), ((1, chans), F32), ((per, chans), F32)]
    semaphores = [
            dma((6,)),
            dma((2, 2)), dma((2, 2)), dma((2, peers)), dma((2, peers)),
            dma((units, chunks)), dma((units, chunks)),
            dma((3, peers * owned)), dma((3, peers * owned)), dma((2, group - 1)), dma((2, group - 1)),
            dma((2, 3)), dma((2, 3)), dma((group - 1,)), dma((group - 1,)),
    ]

    def scoped_kernel(*refs):
        pl.run_scoped(lambda *held: whole_kernel(n, peers, *refs, *held), *semaphores)

    vgrad, ggrad, taps_grad, gain_grad, wgrad = pl.pallas_call(
        scoped_kernel,
        out_shape=[vmem(s, d) for s, d in outs],
        in_specs=[pl.BlockSpec(memory_space=pl.ANY)] * 6,
        out_specs=[pl.BlockSpec(memory_space=vmem)] * len(outs),
        scratch_shapes=[
            vmem((rows, chans), BF16), vmem((rows, chans), BF16), vmem((full, chans), BF16), vmem((rows, chans), BF16),
            vmem((kw, chans), BF16), vmem((1, chans), F32),
            vmem((tiles, kw, LANE), F32),
            vmem((tiles, kw) + block, BF16),
            vmem((tiles, kw, 8, LANE), F32),
            vmem((tiles, rows + 4 * EDGE, LANE), F32),
            vmem((tiles, chunks, TAU + kw - 1) + block, BF16),
            vmem((kw + 1,) + block, BF16),
            vmem((tiles, extent, LANE), F32),
            vmem((tiles, extent, LANE), F32),
            vmem((tiles, extent, LANE), F32),
            vmem((rows, chans), BF16),
            vmem((tiles, extent, LANE), F32),
            vmem((TAU + kw - 1,) + block, BF16),
            vmem((tiles, 2 * TAU) + block, BF16),
            vmem((tiles, CHUNK, LANE), F32),
            vmem((rows, chans), F32),
            vmem((8, chans), F32),
            vmem((n, per, chans), F32),
            vmem((tiles, kw + 1, LANE), F32),
            vmem((2, 2, WIDE, chans), BF16),
            vmem((2, peers, EDGE, chans), BF16),
            vmem((peers - 1, rows, chans), BF16),
            vmem((n // 2, per, chans), BF16),
            vmem((n // 2, per, chans), BF16),
            vmem((n // 4, per, chans), BF16),
            vmem((n // 4, per, chans), BF16),
            vmem((group - 1, per, chans), BF16),
            vmem((group - 1, per, chans), BF16),
            vmem((4,) + piece, BF16),
            vmem((3,) + piece, BF16),
            vmem((4,) + piece, F32),
            vmem(piece, BF16),
            vmem((group,) + piece, BF16),
        ],
        compiler_params=pltpu.CompilerParams(
            collective_id=0, has_side_effects=True, vmem_limit_bytes=52 * 1024 * 1024),
    )(*args)
    vgrad, ggrad, taps_grad, gain_grad, wgrad = finish(vgrad, ggrad, taps_grad, gain_grad, wgrad)
    return vgrad, ggrad, taps_grad, gain_grad.reshape(chans), wgrad


def solution(mesh):
    return jax.shard_map(
        per_device,
        mesh=mesh,
        in_specs=(P("sp", "tp"), P("sp", "tp"), P(None, "tp"), P("tp"), P(None, "tp"), P("sp", "tp")),
        out_specs=(P("sp", "tp"), P("sp", "tp"), P(None, "tp"), P("tp"), P("sp", "tp")),
        check_vma=False,
    )
```

```python
import functools

import jax
import jax.numpy as jnp
from jax import lax
from jax.experimental import pallas as pl
from jax.experimental.pallas import tpu as pltpu
from jax.sharding import PartitionSpec as P

GROUP = 64
EPS = 1e-06
LANE = 128
EDGE = 16
WIDE = 2 * EDGE
SEG = 16
TAU = 8
CHUNK = SEG * TAU
UNIT = 2 * LANE
F32, BF16 = jnp.float32, jnp.bfloat16


def sigmoid(x):
    return 0.5 * jnp.tanh(0.5 * x) + 0.5


def divisor(total, *choices):
    for choice in choices:
        if total % choice == 0:
            return choice
    return total


def group_matrix(stacked):
    row = lax.broadcasted_iota(jnp.int32, (2 * LANE, 2 * LANE), 0)
    col = lax.broadcasted_iota(jnp.int32, (2 * LANE, 2 * LANE), 1)
    if stacked:
        row, col = lax.rem(row, LANE), lax.rem(col, LANE)
    return jnp.where(row // GROUP == col // GROUP, 1.0 / GROUP, 0.0).astype(BF16)


def group_mean(x, stacked):
    high = x.astype(BF16)
    low = (x - high.astype(F32)).astype(BF16)
    return jnp.dot(jnp.concatenate([high, low], axis=1), stacked[:, :LANE], preferred_element_type=F32)


def near_means(x, y, apart):
    both = jnp.dot(jnp.concatenate([x.astype(BF16), y.astype(BF16)], axis=1), apart, preferred_element_type=F32)
    return both[:, :LANE], both[:, LANE:]


def lanes(c):
    return pl.ds(pl.multiple_of(c * LANE, LANE), LANE)


def loop(lo, hi, body):
    def one(i, _):
        body(i)
        return 0

    lax.fori_loop(lo, hi, one, 0)


def put_gated(gated, c, v, g, dst, n):
    gated[c, pl.ds(dst, n), :] = (v.astype(F32) * sigmoid(g.astype(F32))).astype(BF16).astype(F32)


def spread(src, c, low, high, stride):
    half = SEG // 2
    return jnp.concatenate([src[c, pl.ds(low, half, stride=stride), :],
                            src[c, pl.ds(high, half, stride=stride), :]], axis=0).astype(BF16)


def products(pairs):
    sums = [None] * len(pairs)
    for step in zip(*pairs):
        for a, (x, y) in enumerate(step):
            p = x().astype(F32) * y().astype(F32)
            sums[a] = p if sums[a] is None else sums[a] + p
    return sums


def conv_block(kw, source, tapb, c, taus, reverse, put):
    width = min(4, taus)
    for first in range(0, taus, width):
        pairs = []
        for a in range(width):
            tau = first + a
            pairs.append([
                ((lambda j=(tau + kw - 1 - k if reverse else tau + k): source(j)), (lambda k=k: tapb[c, k]))
                for k in range(kw)])
        for a, total in enumerate(products(pairs)):
            put(first + a, total)


def act_to_conv(ng, at, n, own, unit, inv, slope, gain, dconv, gain_part, apart):
    for c in range(unit.shape[0]):
        g = gain[:, c * LANE:(c + 1) * LANE]
        u = unit[c, pl.ds(at, n), :]
        a = ng[:, c * LANE:(c + 1) * LANE] * slope[c, pl.ds(at, n), :]
        au = a * u
        if own:
            gain_part[:, c * LANE:(c + 1) * LANE] += jnp.sum(au.reshape(n // 8, 8, LANE), axis=0)
        h = a * g
        first, second = near_means(h, au * g, apart)
        dconv[c, pl.ds(at, n), :] = inv[c, pl.ds(at, n), :] * (h - first - u * second)


def whole_kernel(n, peers, value_in, gate_in, taps_in, gain_in, weight_in, grad_in,
                 vgrad, ggrad, taps_out, gain_out, wout,
                 value, gate, weight, grad, taps_raw, gain, taps, tapb, tacc,
                 gated, shifted, edges, unit, inv, slope, normed, dconv, dshift, dpack, grow, ngacc,
                 gain_part, wpart, sums,
                 vhalo, ohalo, others, send1, recv1, send2, recv2, send3, recv3,
                 asend, arecv, atotal, zsend, zrecv,
                 lsem, vs, vr, os_, or_, gs, gr, ws, wr, ws3, wr3, as_, ar, as3, ar3):
    rows, chans = value.shape
    tiles = chans // LANE
    kw = taps.shape[1]
    sp, tp = lax.axis_index("sp"), lax.axis_index("tp")
    group = recv3.shape[0] + 1
    b0, b1, zz = lax.rem(sp, 2), lax.rem(sp // 2, 2), sp // 4
    has_left, has_right = sp > 0, sp < n - 1
    left, right = lax.rem(sp + n - 1, n), lax.rem(sp + 1, n)
    mate0 = sp + 1 - 2 * b0
    mate1 = sp + 2 - 4 * b1
    chunks = rows // CHUNK
    owned = chans // UNIT
    units = (peers - 1) * owned

    quarter = lax.rem(sp, 4)

    def plane(d):
        return sp - quarter + lax.rem(quarter + d, 4)

    def zmate(d):
        return lax.rem(sp + 4 * d, n)

    def tmate(j):
        return lax.rem(tp + peers - j, peers)

    def remote(src, dst, s, r, to):
        return pltpu.make_async_remote_copy(
            src_ref=src, dst_ref=dst, send_sem=s, recv_sem=r, device_id=to,
            device_id_type=pl.DeviceIdType.MESH)

    barrier = pltpu.get_barrier_semaphore()

    def hello(friend):
        pl.semaphore_signal(barrier, inc=1, device_id=friend, device_id_type=pl.DeviceIdType.MESH)

    friends = [(sp, tmate(j)) for j in range(1, peers)] + [(plane(d), tp) for d in range(1, 4)]
    friends += [(zmate(d), tp) for d in range(1, group)]
    for friend in friends:
        hello(friend)

    @pl.when(has_left)
    def _():
        for j in range(peers):
            hello((left, tmate(j)))

    @pl.when(has_right)
    def _():
        for j in range(peers):
            hello((right, tmate(j)))

    loads = [pltpu.make_async_copy(src, dst, lsem.at[i]) for i, (src, dst) in enumerate(
        ((grad_in, grad), (value_in, value), (gate_in, gate), (taps_in, taps_raw), (gain_in, gain), (weight_in, weight)))]
    loads = loads[1:3] + loads[:1] + loads[3:]
    for copy in loads:
        copy.start()
    pl.semaphore_wait(barrier, len(friends) + peers * (has_left.astype(jnp.int32) + has_right.astype(jnp.int32)))

    halos = [[remote(ref.at[pl.ds(start, WIDE)], vhalo.at[side, i], vs.at[side, i], vr.at[side, i], (to, tp))
              for i, ref in enumerate((value_in, gate_in))]
             for side, (start, to) in enumerate(((rows - WIDE, right), (0, left)))]
    ohalos = [[remote(grad_in.at[pl.ds(start, EDGE)], ohalo.at[side, j], os_.at[side, j], or_.at[side, j], (to, tmate(j)))
               for j in range(peers)]
              for side, (start, to) in enumerate(((rows - EDGE, right), (0, left)))]
    sends = (has_right, has_left)
    arrives = (has_left, has_right)

    def unit_lane(p):
        p = lax.rem(p, owned)
        return pl.multiple_of(jnp.where(2 * tp < peers, p, owned - 1 - p) * UNIT, UNIT)

    def gather(p, r):
        j = p // owned + 1
        at = (pl.ds(pl.multiple_of(r * CHUNK, CHUNK), CHUNK), pl.ds(unit_lane(p), UNIT))
        return remote(grad_in.at[at], others.at[(j - 1,) + at], gs.at[p, r], gr.at[p, r], (sp, tmate(j)))

    def start_halos(copies):
        for side in range(2):
            @pl.when(sends[side])
            def _(side=side):
                for copy in copies[side]:
                    copy.start()

    def unit_lane_from(p):
        j = p // owned + 1
        sender = lax.rem(tp + j, peers)
        q = lax.rem(p, owned)
        return pl.multiple_of(jnp.where(2 * sender < peers, q, owned - 1 - q) * UNIT, UNIT)

    start_halos(halos)
    for p in range(units):
        for r in range(chunks):
            gather(p, r).start()

    stacked, apart = group_matrix(True), group_matrix(False)
    loads[3].wait()
    for c in range(tiles):
        taps[c] = taps_raw[:, c * LANE:(c + 1) * LANE].astype(F32)

    def widen(c):
        for k in range(kw):
            tapb[c, k] = jnp.broadcast_to(taps[c, pl.ds(k, 1), :], (SEG, LANE)).astype(BF16)

    loop(0, tiles, widen)
    gain_part[...] = jnp.zeros_like(gain_part)
    tacc[...] = jnp.zeros_like(tacc)
    loads[0].wait()
    loads[1].wait()
    gstep = divisor(rows, 256, 32)

    def own_gated(c):
        def chunk(r):
            at = pl.multiple_of(r * gstep, gstep)
            put_gated(gated, c, value[pl.ds(at, gstep), lanes(c)], gate[pl.ds(at, gstep), lanes(c)],
                      pl.multiple_of(at + WIDE, 8), gstep)

        loop(0, rows // gstep, chunk)

    loop(0, tiles, own_gated)

    def put_halos():
        for side, dst in ((0, 0), (1, rows + WIDE)):
            @pl.when(arrives[side])
            def _(side=side, dst=dst):
                for copy in halos[side]:
                    copy.wait_recv()

                def one(c):
                    put_gated(gated, c, vhalo[side, 0, :, lanes(c)], vhalo[side, 1, :, lanes(c)], dst, WIDE)

                loop(0, tiles, one)

            @pl.when(jnp.logical_not(arrives[side]))
            def _(dst=dst):
                for c in range(tiles):
                    gated[c, pl.ds(dst, WIDE), :] = jnp.zeros((WIDE, LANE), F32)

    def forward(i):
        r = lax.rem(i + 1, chunks)
        base = r * CHUNK

        @pl.when(i == chunks - 2)
        def _():
            put_halos()

        def tile(c):
            for j in range(TAU + kw - 1):
                low = base + (j + WIDE - kw // 2)
                shifted[c, r, j] = spread(gated, c, low, low + TAU * (SEG // 2), TAU)

            def put(tau, total):
                for h in range(2):
                    start = base + (EDGE + tau + h * TAU * (SEG // 2))
                    unit[c, pl.ds(start, SEG // 2, stride=TAU), :] = total[h * (SEG // 2):(h + 1) * (SEG // 2)]

            conv_block(kw, lambda j: shifted[c, r, j], tapb, c, TAU, False, put)

        loop(0, tiles, tile)

    loop(0, chunks, forward)

    def forward_edges(c):
        for j in range(2 + kw - 1):
            edges[j] = spread(gated, c, EDGE - kw // 2 + j, rows + WIDE - kw // 2 + j, 2)

        def put(tau, total):
            for h, start in ((0, tau), (1, rows + EDGE + tau)):
                unit[c, pl.ds(start, SEG // 2, stride=2), :] = total[h * (SEG // 2):(h + 1) * (SEG // 2)]

        conv_block(kw, lambda j: edges[j], tapb, c, 2, False, put)

    loop(0, tiles, forward_edges)
    loads[4].wait()

    def norm_rows(at, count, own):
        xs = [unit[c, pl.ds(at, count), :] for c in range(tiles)]
        centred = [x - group_mean(x, stacked) for x in xs]
        for c in range(0, tiles, 2):
            spreads = near_means(centred[c] * centred[c], centred[c + 1] * centred[c + 1], apart)
            for e, var in zip((c, c + 1), spreads):
                rs = lax.rsqrt(var + EPS)
                inv[e, pl.ds(at, count), :] = rs
                u = centred[e] * rs
                unit[e, pl.ds(at, count), :] = u
                p = u * gain[:, e * LANE:(e + 1) * LANE]
                s = sigmoid(p)
                slope[e, pl.ds(at, count), :] = s * (1.0 + p * (1.0 - s))
                if own is not None:
                    normed[pl.ds(own, count), e * LANE:(e + 1) * LANE] = (p * s).astype(BF16)

    def norm(r):
        at = pl.multiple_of(r * CHUNK, CHUNK)
        norm_rows(pl.multiple_of(at + EDGE, 8), CHUNK, at)

    loop(0, chunks, norm)
    norm_rows(0, EDGE, None)
    norm_rows(rows + EDGE, EDGE, None)
    nstep = divisor(rows, 256, 32)

    def owner(j):
        return lax.rem(tp + j, peers)

    per = wpart.shape[1]
    span = UNIT // per

    def unit_of(j, p):
        lane = unit_lane_from((j - 1) * owned + p) if j else pl.multiple_of(p * UNIT, UNIT)
        return lane, (owner(j) * chans + lane) // per

    def weight_part(j, p, first, count, add):
        lane, base = unit_of(j, p)
        at = (pl.ds(first, count), pl.ds(lane, UNIT))
        lhs = others[(j - 1,) + at] if j else grad[at]
        out = lax.dot_general(lhs, normed[pl.ds(first, count), :], (((0,), (0,)), ((), ())), preferred_element_type=F32)
        out = out.reshape(span, per, chans)
        wpart[pl.ds(base, span)] = wpart[pl.ds(base, span)] + out if add else out

    pairs, quads, far = span // 2, span // 4, span // 4

    def half1(j, p):
        at = pl.ds(unit_of(j, p)[1] // 2, pairs)
        k = j * owned + p
        return remote(send1.at[at], recv1.at[at], ws.at[0, k], wr.at[0, k], (mate0, tp))

    half = chans // 2

    def cols(h):
        return pl.ds(h * half, half)

    def half2(j, p, h):
        at = (pl.ds(unit_of(j, p)[1] // 4, quads), slice(None), cols(h))
        k = j * owned + p
        return remote(send2.at[at], recv2.at[at], ws.at[1 + h, k], wr.at[1 + h, k], (mate1, tp))

    def start1(j, p):
        first = unit_of(j, p)[1] // 2

        def cast(i):
            send1[first + i] = wpart[2 * (first + i) + 1 - b0].astype(BF16)

        loop(0, pairs, cast)
        half1(j, p).start()

    def start2(j, p):
        first = unit_of(j, p)[1] // 4
        half1(j, p).wait_recv()
        for h in range(2):
            def cast(i, h=h):
                other = 2 * (first + i) + 1 - b1
                send2[first + i, :, cols(h)] = (
                    wpart[2 * other + b0, :, cols(h)] + recv1[other, :, cols(h)].astype(F32)).astype(BF16)

            loop(0, quads, cast)
            half2(j, p, h).start()

        def keep(i):
            mine = 2 * (first + i) + b1
            wpart[2 * mine + b0] = wpart[2 * mine + b0] + recv1[mine].astype(F32)

        loop(0, quads, keep)

    def total2(z, h):
        return wpart[4 * z + 2 * b1 + b0, :, cols(h)] + recv2[z, :, cols(h)].astype(F32)

    def final_copy(slot, h):
        at = (slot, slice(None), cols(h))
        return remote(send3.at[at], recv3.at[at], ws3.at[h, slot], wr3.at[h, slot],
                      (lax.rem(sp + 4 * (slot + 1), n), tp))

    def start3(j, p, h):
        half2(j, p, h).wait_recv()
        first = unit_of(j, p)[1] // 4

        def one(i):
            z = first + i
            d = lax.rem(z + group - zz, group)

            @pl.when(d != 0)
            def _():
                send3[d - 1, :, cols(h)] = total2(z, h).astype(BF16)
                final_copy(d - 1, h).start()

        loop(0, far, one)

    def weight_rows(j, lane):
        return pl.ds(pl.multiple_of(owner(j) * chans + lane, UNIT), UNIT)

    def own_ng(r):
        at = pl.ds(pl.multiple_of(r * nstep, nstep), nstep)
        ngacc[at, :] = jnp.dot(grad[at, :], weight[pl.ds(pl.multiple_of(owner(0) * chans, UNIT), chans), :],
                               preferred_element_type=F32)

    def unit_ng(p):
        def add(r):
            at = pl.ds(pl.multiple_of(r * nstep, nstep), nstep)
            lane = unit_lane_from(p)
            j = p // owned + 1
            ngacc[at, :] += jnp.dot(others[j - 1, at, pl.ds(lane, UNIT)], weight[weight_rows(j, lane), :],
                                    preferred_element_type=F32)

        loop(0, rows // nstep, add)

    def middle(r):
        at = pl.ds(pl.multiple_of(r * CHUNK, CHUNK), CHUNK)
        ng = ngacc[at, :] + jnp.dot(others[peers - 2, at, :], weight[pl.ds(pl.multiple_of(owner(peers - 1) * chans, UNIT), chans), :],
                                    preferred_element_type=F32)
        act_to_conv(ng, pl.multiple_of(r * CHUNK + EDGE, 8), CHUNK, True, unit, inv, slope, gain, dconv, gain_part, apart)

    def taps_chunks(*rs):
        def tile(c):
            for i, r in enumerate(rs):
                for tau in range(TAU):
                    low = r * CHUNK + (EDGE + tau)
                    dpack[c, i * TAU + tau] = spread(dconv, c, low, low + TAU * (SEG // 2), TAU)
            for k0 in range(0, kw, 4):
                ks = range(k0, min(k0 + 4, kw))
                pairs_ = [[((lambda r=r, j=tau + k: shifted[c, r, j]), (lambda i=i, tau=tau: dpack[c, i * TAU + tau]))
                           for i, r in enumerate(rs) for tau in range(TAU)] for k in ks]
                for k, total in zip(ks, products(pairs_)):
                    tacc[c, k] += total[:SEG // 2] + total[SEG // 2:]

        loop(0, tiles, tile)

    def finalize(r):
        gather(units - 1, r).wait_recv()
        middle(r)

    def finalize_two(i):
        finalize(2 * i)
        finalize(2 * i + 1)
        taps_chunks(2 * i, 2 * i + 1)

    def fold_taps(c):
        for k in range(kw):
            sums[c, pl.ds(k, 1), :] = jnp.sum(tacc[c, k], axis=0, keepdims=True)
        sums[c, pl.ds(kw, 1), :] = jnp.sum(gain_part[:, lanes(c)], axis=0, keepdims=True)

    def edge_conv():
        for side, at in ((0, 0), (1, rows + EDGE)):
            @pl.when(arrives[side])
            def _(side=side, at=at):
                for copy in ohalos[side]:
                    copy.wait_recv()
                ng = sum(jnp.dot(ohalo[side, j], weight[pl.ds(pl.multiple_of(owner(j) * chans, UNIT), chans), :],
                                 preferred_element_type=F32) for j in range(peers))
                act_to_conv(ng, at, EDGE, False, unit, inv, slope, gain, dconv, gain_part, apart)

            @pl.when(jnp.logical_not(arrives[side]))
            def _(at=at):
                for c in range(tiles):
                    dconv[c, pl.ds(at, EDGE), :] = jnp.zeros((EDGE, LANE), F32)

    def backward(r):
        def tile(c):
            base = r * CHUNK
            for j in range(TAU + kw - 1):
                low = base + (EDGE - kw // 2 + j)
                dshift[j] = spread(dconv, c, low, low + TAU * (SEG // 2), TAU)

            def put(tau, total):
                for h in range(2):
                    grow[c, pl.ds(tau + h * TAU * (SEG // 2), SEG // 2, stride=TAU), :] = (
                        total[h * (SEG // 2):(h + 1) * (SEG // 2)])

            conv_block(kw, lambda j: dshift[j], tapb, c, TAU, True, put)
            at = pl.ds(pl.multiple_of(base, CHUNK), CHUNK)
            s = sigmoid(gate[at, lanes(c)].astype(F32))
            v = value[at, lanes(c)].astype(F32)
            out = grow[c] * s
            vgrad[at, lanes(c)] = out.astype(BF16)
            ggrad[at, lanes(c)] = (out * v * (1.0 - s)).astype(BF16)

        loop(0, tiles, tile)

    part = (kw + 1) // 2
    collects = b0 == 1

    def collector(q):
        return sp - quarter + 2 * q + 1

    def gather_sums(q, sender):
        return remote(asend.at[q], arecv.at[sender], as_.at[0, q], ar.at[0, sender], (collector(q), tp))

    def other(d):
        return lax.rem(quarter + d, 4)

    def share(d):
        return remote(atotal.at[b1], atotal.at[b1], as_.at[1, d - 1], ar.at[1, b1], (plane(d), tp))

    def spread_sums(d):
        return remote(zsend, zrecv.at[zz], as3.at[d - 1], ar3.at[d - 1], (zmate(d), tp))

    def shared(q):
        return remote(atotal.at[q], atotal.at[q], as_.at[1, 0], ar.at[1, q], (plane(1), tp))

    loads[2].wait()
    for p in range(owned):
        weight_part(0, p, 0, rows, False)
        start1(0, p)
    loads[5].wait()
    loop(0, rows // nstep, own_ng)
    for p in range(owned):
        start2(0, p)
    for p in range(units - 1):
        for r in range(chunks):
            gather(p, r).wait_recv()
        weight_part(p // owned + 1, p % owned, 0, rows, False)
        start1(p // owned + 1, p % owned)
        if p < units - owned:
            unit_ng(p)
    for p in range(owned):
        for h in range(2):
            start3(0, p, h)
    for p in range(units - 1):
        start2(p // owned + 1, p % owned)
    lj, lp = peers - 1, owned - 1
    loop(0, 2, finalize_two)
    for p in range(units - 1):
        for h in range(2):
            start3(p // owned + 1, p % owned, h)
    loop(2, chunks // 2 - 1, finalize_two)
    weight_part(lj, lp, 0, rows - 2 * CHUNK, False)
    finalize(chunks - 2)
    taps_chunks(chunks - 2)
    gather(units - 1, chunks - 1).wait_recv()
    middle(chunks - 1)
    taps_chunks(chunks - 1)
    loop(0, tiles, fold_taps)
    for q in range(2):
        asend[q] = sums[:, q * part:(q + 1) * part, :].astype(BF16)

        @pl.when(quarter != 2 * q + 1)
        def _(q=q):
            gather_sums(q, quarter).start()

    start_halos(ohalos)
    weight_part(lj, lp, rows - 2 * CHUNK, 2 * CHUNK, True)
    start1(lj, lp)
    loop(1, 3, backward)
    start2(lj, lp)
    backward(3)

    @pl.when(collects)
    def _():
        for d in range(1, 4):
            gather_sums(0, other(d)).wait_recv()
        mine = sums[:, pl.ds(pl.multiple_of(b1 * part, part), part), :]
        for d in range(1, 4):
            mine += arecv[other(d)].astype(F32)
        zsend[...] = mine.astype(BF16)
        for d in range(1, group):
            spread_sums(d).start()

    loop(4, chunks - 1, backward)
    edge_conv()
    start3(lj, lp, 0)
    backward(0)
    start3(lj, lp, 1)

    @pl.when(collects)
    def _():
        zrecv[zz] = zsend[...]
        for d in range(1, group):
            peer = lax.rem(zz + group - d, group)
            remote(zsend, zrecv.at[peer], as3.at[d - 1], ar3.at[d - 1], (zmate(d), tp)).wait_recv()
        total = zrecv[0].astype(F32)
        for z in range(1, group):
            total += zrecv[z].astype(F32)
        atotal[b1] = total
        for d in (1, 3, 2):
            share(d).start()

    backward(chunks - 1)
    for h in range(2):
        final = total2(zz, h)
        for d in range(1, group):
            final_copy(d - 1, h).wait_recv()
            final += recv3[d - 1, :, cols(h)].astype(F32)
        wout[:, cols(h)] = final
    for q in range(2):
        @pl.when(quarter != 2 * q + 1)
        def _(q=q):
            shared(q).wait_recv()

    for c in range(tiles):
        tot = jnp.concatenate([atotal[q, c] for q in range(2)], axis=0)
        taps_out[:, c * LANE:(c + 1) * LANE] = tot[:kw]
        gain_out[:, c * LANE:(c + 1) * LANE] = tot[kw:]
    for q in range(2):
        @pl.when(quarter != 2 * q + 1)
        def _(q=q):
            gather_sums(q, quarter).wait_send()

    @pl.when(collects)
    def _():
        for d in range(1, 4):
            share(d).wait_send()
        for d in range(1, group):
            spread_sums(d).wait_send()

    for side in range(2):
        @pl.when(sends[side])
        def _(side=side):
            for copy in halos[side] + ohalos[side]:
                copy.wait_send()
    for p in range(units):
        for r in range(chunks):
            gather(p, r).wait_send()
    for j in range(peers):
        for p in range(owned):
            half1(j, p).wait_send()
            for h in range(2):
                half2(j, p, h).wait_send()
    for d in range(1, group):
        for h in range(2):
            final_copy(d - 1, h).wait_send()


def finish_kernel(parts, *refs):
    count = len(parts)
    sources, targets = refs[:count], refs[count:]

    def move(osem):
        outgoing = []
        for src, dst, pieces in zip(sources, targets, parts):
            size = src.shape[0] // pieces
            for p in range(pieces):
                at = pl.ds(p * size, size)
                outgoing.append(pltpu.make_async_copy(src.at[at], dst.at[at], osem.at[len(outgoing)]))
        for copy in outgoing:
            copy.start()
        for copy in outgoing:
            copy.wait()

    pl.run_scoped(move, pltpu.SemaphoreType.DMA((sum(parts),)))


def finish(*arrays):
    parts = [4 if a.shape[0] % 128 == 0 else 1 for a in arrays]
    return pl.pallas_call(
        functools.partial(finish_kernel, parts),
        out_shape=[jax.ShapeDtypeStruct(a.shape, a.dtype) for a in arrays],
        in_specs=[pl.BlockSpec(memory_space=pltpu.VMEM)] * len(arrays),
        out_specs=[pl.BlockSpec(memory_space=pl.ANY)] * len(arrays),
    )(*[pltpu.with_memory_space_constraint(a, pltpu.VMEM) for a in arrays])


def per_device(value, gate, conv_taps, norm_gain, point_weight, out_grad):
    rows, chans = value.shape
    kw = conv_taps.shape[0]
    tiles = chans // LANE
    n, peers = lax.axis_size("sp"), lax.axis_size("tp")
    extent = rows + WIDE
    full = point_weight.shape[0]
    per = full // n
    group = n // 4
    chunks = rows // CHUNK
    owned = chans // UNIT
    units = (peers - 1) * owned
    gain = norm_gain.reshape(1, chans)
    args = (value, gate, conv_taps, gain, point_weight, out_grad)
    piece = (tiles, (kw + 1) // 2, LANE)
    vmem, dma = pltpu.VMEM, pltpu.SemaphoreType.DMA
    block = (SEG, LANE)
    outs = [((rows, chans), BF16), ((rows, chans), BF16), ((kw, chans), F32), ((1, chans), F32), ((per, chans), F32)]
    semaphores = [
            dma((6,)),
            dma((2, 2)), dma((2, 2)), dma((2, peers)), dma((2, peers)),
            dma((units, chunks)), dma((units, chunks)),
            dma((3, peers * owned)), dma((3, peers * owned)), dma((2, group - 1)), dma((2, group - 1)),
            dma((2, 3)), dma((2, 4)), dma((group - 1,)), dma((group - 1,)),
    ]

    def scoped_kernel(*refs):
        pl.run_scoped(lambda *held: whole_kernel(n, peers, *refs, *held), *semaphores)

    vgrad, ggrad, taps_grad, gain_grad, wgrad = pl.pallas_call(
        scoped_kernel,
        out_shape=[vmem(s, d) for s, d in outs],
        in_specs=[pl.BlockSpec(memory_space=pl.ANY)] * 6,
        out_specs=[pl.BlockSpec(memory_space=vmem)] * len(outs),
        scratch_shapes=[
            vmem((rows, chans), BF16), vmem((rows, chans), BF16), vmem((full, chans), BF16), vmem((rows, chans), BF16),
            vmem((kw, chans), BF16), vmem((1, chans), F32),
            vmem((tiles, kw, LANE), F32),
            vmem((tiles, kw) + block, BF16),
            vmem((tiles, kw, 8, LANE), F32),
            vmem((tiles, rows + 4 * EDGE, LANE), F32),
            vmem((tiles, chunks, TAU + kw - 1) + block, BF16),
            vmem((kw + 1,) + block, BF16),
            vmem((tiles, extent, LANE), F32),
            vmem((tiles, extent, LANE), F32),
            vmem((tiles, extent, LANE), F32),
            vmem((rows, chans), BF16),
            vmem((tiles, extent, LANE), F32),
            vmem((TAU + kw - 1,) + block, BF16),
            vmem((tiles, 2 * TAU) + block, BF16),
            vmem((tiles, CHUNK, LANE), F32),
            vmem((rows, chans), F32),
            vmem((8, chans), F32),
            vmem((n, per, chans), F32),
            vmem((tiles, kw + 1, LANE), F32),
            vmem((2, 2, WIDE, chans), BF16),
            vmem((2, peers, EDGE, chans), BF16),
            vmem((peers - 1, rows, chans), BF16),
            vmem((n // 2, per, chans), BF16),
            vmem((n // 2, per, chans), BF16),
            vmem((n // 4, per, chans), BF16),
            vmem((n // 4, per, chans), BF16),
            vmem((group - 1, per, chans), BF16),
            vmem((group - 1, per, chans), BF16),
            vmem((2,) + piece, BF16),
            vmem((4,) + piece, BF16),
            vmem((2,) + piece, F32),
            vmem(piece, BF16),
            vmem((group,) + piece, BF16),
        ],
        compiler_params=pltpu.CompilerParams(
            collective_id=0, has_side_effects=True, vmem_limit_bytes=52 * 1024 * 1024),
    )(*args)
    vgrad, ggrad, taps_grad, gain_grad, wgrad = finish(vgrad, ggrad, taps_grad, gain_grad, wgrad)
    return vgrad, ggrad, taps_grad, gain_grad.reshape(chans), wgrad


def solution(mesh):
    return jax.shard_map(
        per_device,
        mesh=mesh,
        in_specs=(P("sp", "tp"), P("sp", "tp"), P(None, "tp"), P("tp"), P(None, "tp"), P("sp", "tp")),
        out_specs=(P("sp", "tp"), P("sp", "tp"), P(None, "tp"), P("tp"), P("sp", "tp")),
        check_vma=False,
    )
```

```python
import functools

import jax
import jax.numpy as jnp
from jax import lax
from jax.experimental import pallas as pl
from jax.experimental.pallas import tpu as pltpu
from jax.sharding import PartitionSpec as P

GROUP = 64
EPS = 1e-06
LANE = 128
EDGE = 16
WIDE = 2 * EDGE
SEG = 16
TAU = 8
CHUNK = SEG * TAU
UNIT = 2 * LANE
F32, BF16 = jnp.float32, jnp.bfloat16


def sigmoid(x):
    return 0.5 * jnp.tanh(0.5 * x) + 0.5


def divisor(total, *choices):
    for choice in choices:
        if total % choice == 0:
            return choice
    return total


def group_matrix(stacked):
    row = lax.broadcasted_iota(jnp.int32, (2 * LANE, 2 * LANE), 0)
    col = lax.broadcasted_iota(jnp.int32, (2 * LANE, 2 * LANE), 1)
    if stacked:
        row, col = lax.rem(row, LANE), lax.rem(col, LANE)
    return jnp.where(row // GROUP == col // GROUP, 1.0 / GROUP, 0.0).astype(BF16)


def group_mean(x, stacked):
    high = x.astype(BF16)
    low = (x - high.astype(F32)).astype(BF16)
    return jnp.dot(jnp.concatenate([high, low], axis=1), stacked[:, :LANE], preferred_element_type=F32)


def near_means(x, y, apart):
    both = jnp.dot(jnp.concatenate([x.astype(BF16), y.astype(BF16)], axis=1), apart, preferred_element_type=F32)
    return both[:, :LANE], both[:, LANE:]


def lanes(c):
    return pl.ds(pl.multiple_of(c * LANE, LANE), LANE)


def loop(lo, hi, body):
    def one(i, _):
        body(i)
        return 0

    lax.fori_loop(lo, hi, one, 0)


def put_gated(gated, c, v, g, dst, n):
    gated[c, pl.ds(dst, n), :] = (v.astype(F32) * sigmoid(g.astype(F32))).astype(BF16).astype(F32)


def spread(src, c, low, high, stride):
    half = SEG // 2
    return jnp.concatenate([src[c, pl.ds(low, half, stride=stride), :],
                            src[c, pl.ds(high, half, stride=stride), :]], axis=0).astype(BF16)


def products(pairs):
    sums = [None] * len(pairs)
    for step in zip(*pairs):
        for a, (x, y) in enumerate(step):
            p = x().astype(F32) * y().astype(F32)
            sums[a] = p if sums[a] is None else sums[a] + p
    return sums


def conv_block(kw, source, tapb, c, taus, reverse, put):
    width = min(4, taus)
    for first in range(0, taus, width):
        pairs = []
        for a in range(width):
            tau = first + a
            pairs.append([
                ((lambda j=(tau + kw - 1 - k if reverse else tau + k): source(j)), (lambda k=k: tapb[c, k]))
                for k in range(kw)])
        for a, total in enumerate(products(pairs)):
            put(first + a, total)


def act_to_conv(ng, at, n, own, unit, inv, slope, gain, dconv, gain_part, apart):
    for c in range(unit.shape[0]):
        g = gain[:, c * LANE:(c + 1) * LANE]
        u = unit[c, pl.ds(at, n), :]
        a = ng[:, c * LANE:(c + 1) * LANE] * slope[c, pl.ds(at, n), :]
        au = a * u
        if own:
            gain_part[:, c * LANE:(c + 1) * LANE] += jnp.sum(au.reshape(n // 8, 8, LANE), axis=0)
        h = a * g
        first, second = near_means(h, au * g, apart)
        dconv[c, pl.ds(at, n), :] = inv[c, pl.ds(at, n), :] * (h - first - u * second)


def whole_kernel(n, peers, value_in, gate_in, taps_in, gain_in, weight_in, grad_in,
                 vgrad, ggrad, taps_out, gain_out, wout,
                 value, gate, weight, grad, taps_raw, gain, taps, tapb, tacc,
                 gated, shifted, edges, unit, inv, slope, normed, dconv, dshift, dpack, grow, ngacc,
                 gain_part, wpart, sums,
                 vhalo, ohalo, others, send1, recv1, send2, recv2, send3, recv3,
                 asend, arecv, atotal, zsend, zrecv,
                 lsem, vs, vr, os_, or_, gs, gr, ws, wr, ws3, wr3, as_, ar, as3, ar3):
    rows, chans = value.shape
    tiles = chans // LANE
    kw = taps.shape[1]
    sp, tp = lax.axis_index("sp"), lax.axis_index("tp")
    group = recv3.shape[0] + 1
    b0, b1, zz = lax.rem(sp, 2), lax.rem(sp // 2, 2), sp // 4
    has_left, has_right = sp > 0, sp < n - 1
    left, right = lax.rem(sp + n - 1, n), lax.rem(sp + 1, n)
    mate0 = sp + 1 - 2 * b0
    mate1 = sp + 2 - 4 * b1
    chunks = rows // CHUNK
    owned = chans // UNIT
    units = (peers - 1) * owned

    quarter = lax.rem(sp, 4)

    def plane(d):
        return sp - quarter + lax.rem(quarter + d, 4)

    def zmate(d):
        return lax.rem(sp + 4 * d, n)

    def tmate(j):
        return lax.rem(tp + peers - j, peers)

    def remote(src, dst, s, r, to):
        return pltpu.make_async_remote_copy(
            src_ref=src, dst_ref=dst, send_sem=s, recv_sem=r, device_id=to,
            device_id_type=pl.DeviceIdType.MESH)

    barrier = pltpu.get_barrier_semaphore()

    def hello(friend):
        pl.semaphore_signal(barrier, inc=1, device_id=friend, device_id_type=pl.DeviceIdType.MESH)

    friends = [(sp, tmate(j)) for j in range(1, peers)] + [(plane(d), tp) for d in range(1, 4)]
    friends += [(zmate(d), tp) for d in range(1, group)]
    for friend in friends:
        hello(friend)

    @pl.when(has_left)
    def _():
        for j in range(peers):
            hello((left, tmate(j)))

    @pl.when(has_right)
    def _():
        for j in range(peers):
            hello((right, tmate(j)))

    loads = [pltpu.make_async_copy(src, dst, lsem.at[i]) for i, (src, dst) in enumerate(
        ((grad_in, grad), (value_in, value), (gate_in, gate), (taps_in, taps_raw), (gain_in, gain), (weight_in, weight)))]
    loads = loads[1:3] + loads[:1] + loads[3:]
    for copy in loads:
        copy.start()
    pl.semaphore_wait(barrier, len(friends) + peers * (has_left.astype(jnp.int32) + has_right.astype(jnp.int32)))

    halos = [[remote(ref.at[pl.ds(start, WIDE)], vhalo.at[side, i], vs.at[side, i], vr.at[side, i], (to, tp))
              for i, ref in enumerate((value_in, gate_in))]
             for side, (start, to) in enumerate(((rows - WIDE, right), (0, left)))]
    ohalos = [[remote(grad_in.at[pl.ds(start, EDGE)], ohalo.at[side, j], os_.at[side, j], or_.at[side, j], (to, tmate(j)))
               for j in range(peers)]
              for side, (start, to) in enumerate(((rows - EDGE, right), (0, left)))]
    sends = (has_right, has_left)
    arrives = (has_left, has_right)

    def unit_lane(p):
        p = lax.rem(p, owned)
        return pl.multiple_of(jnp.where(2 * tp < peers, p, owned - 1 - p) * UNIT, UNIT)

    def gather(p, r):
        j = p // owned + 1
        at = (pl.ds(pl.multiple_of(r * CHUNK, CHUNK), CHUNK), pl.ds(unit_lane(p), UNIT))
        return remote(grad_in.at[at], others.at[(j - 1,) + at], gs.at[p, r], gr.at[p, r], (sp, tmate(j)))

    def start_halos(copies):
        for side in range(2):
            @pl.when(sends[side])
            def _(side=side):
                for copy in copies[side]:
                    copy.start()

    def unit_lane_from(p):
        j = p // owned + 1
        sender = lax.rem(tp + j, peers)
        q = lax.rem(p, owned)
        return pl.multiple_of(jnp.where(2 * sender < peers, q, owned - 1 - q) * UNIT, UNIT)

    start_halos(halos)
    held = range(chunks - 2, chunks)

    def start_held():
        for r in held:
            gather(units - 1, r).start()

    for p in range(units):
        for r in range(chunks):
            if p < units - 1 or r not in held:
                gather(p, r).start()
    pl.when(b0 == 0)(start_held)

    stacked, apart = group_matrix(True), group_matrix(False)
    loads[3].wait()
    for c in range(tiles):
        taps[c] = taps_raw[:, c * LANE:(c + 1) * LANE].astype(F32)

    def widen(c):
        for k in range(kw):
            tapb[c, k] = jnp.broadcast_to(taps[c, pl.ds(k, 1), :], (SEG, LANE)).astype(BF16)

    loop(0, tiles, widen)
    gain_part[...] = jnp.zeros_like(gain_part)
    tacc[...] = jnp.zeros_like(tacc)
    loads[0].wait()
    loads[1].wait()
    gstep = divisor(rows, 256, 32)

    def own_gated(c):
        def chunk(r):
            at = pl.multiple_of(r * gstep, gstep)
            put_gated(gated, c, value[pl.ds(at, gstep), lanes(c)], gate[pl.ds(at, gstep), lanes(c)],
                      pl.multiple_of(at + WIDE, 8), gstep)

        loop(0, rows // gstep, chunk)

    loop(0, tiles, own_gated)

    def put_halos():
        for side, dst in ((0, 0), (1, rows + WIDE)):
            @pl.when(arrives[side])
            def _(side=side, dst=dst):
                for copy in halos[side]:
                    copy.wait_recv()

                def one(c):
                    put_gated(gated, c, vhalo[side, 0, :, lanes(c)], vhalo[side, 1, :, lanes(c)], dst, WIDE)

                loop(0, tiles, one)

            @pl.when(jnp.logical_not(arrives[side]))
            def _(dst=dst):
                for c in range(tiles):
                    gated[c, pl.ds(dst, WIDE), :] = jnp.zeros((WIDE, LANE), F32)

    def forward(i):
        r = lax.rem(i + 1, chunks)
        base = r * CHUNK

        @pl.when(i == chunks - 2)
        def _():
            put_halos()

        def tile(c):
            for j in range(TAU + kw - 1):
                low = base + (j + WIDE - kw // 2)
                shifted[c, r, j] = spread(gated, c, low, low + TAU * (SEG // 2), TAU)

            def put(tau, total):
                for h in range(2):
                    start = base + (EDGE + tau + h * TAU * (SEG // 2))
                    unit[c, pl.ds(start, SEG // 2, stride=TAU), :] = total[h * (SEG // 2):(h + 1) * (SEG // 2)]

            conv_block(kw, lambda j: shifted[c, r, j], tapb, c, TAU, False, put)

        loop(0, tiles, tile)

    loop(0, chunks, forward)

    def forward_edges(c):
        for j in range(2 + kw - 1):
            edges[j] = spread(gated, c, EDGE - kw // 2 + j, rows + WIDE - kw // 2 + j, 2)

        def put(tau, total):
            for h, start in ((0, tau), (1, rows + EDGE + tau)):
                unit[c, pl.ds(start, SEG // 2, stride=2), :] = total[h * (SEG // 2):(h + 1) * (SEG // 2)]

        conv_block(kw, lambda j: edges[j], tapb, c, 2, False, put)

    loop(0, tiles, forward_edges)
    loads[4].wait()

    def norm_rows(at, count, own):
        xs = [unit[c, pl.ds(at, count), :] for c in range(tiles)]
        centred = [x - group_mean(x, stacked) for x in xs]
        for c in range(0, tiles, 2):
            spreads = near_means(centred[c] * centred[c], centred[c + 1] * centred[c + 1], apart)
            for e, var in zip((c, c + 1), spreads):
                rs = lax.rsqrt(var + EPS)
                inv[e, pl.ds(at, count), :] = rs
                u = centred[e] * rs
                unit[e, pl.ds(at, count), :] = u
                p = u * gain[:, e * LANE:(e + 1) * LANE]
                s = sigmoid(p)
                slope[e, pl.ds(at, count), :] = s * (1.0 + p * (1.0 - s))
                if own is not None:
                    normed[pl.ds(own, count), e * LANE:(e + 1) * LANE] = (p * s).astype(BF16)

    def norm(r):
        at = pl.multiple_of(r * CHUNK, CHUNK)
        norm_rows(pl.multiple_of(at + EDGE, 8), CHUNK, at)

    loop(0, chunks, norm)
    norm_rows(0, EDGE, None)
    norm_rows(rows + EDGE, EDGE, None)
    nstep = divisor(rows, 256, 32)

    def owner(j):
        return lax.rem(tp + j, peers)

    per = wpart.shape[1]
    span = UNIT // per

    def unit_of(j, p):
        lane = unit_lane_from((j - 1) * owned + p) if j else pl.multiple_of(p * UNIT, UNIT)
        return lane, (owner(j) * chans + lane) // per

    def weight_part(j, p, first, count, add):
        lane, base = unit_of(j, p)
        at = (pl.ds(first, count), pl.ds(lane, UNIT))
        lhs = others[(j - 1,) + at] if j else grad[at]
        out = lax.dot_general(lhs, normed[pl.ds(first, count), :], (((0,), (0,)), ((), ())), preferred_element_type=F32)
        out = out.reshape(span, per, chans)
        wpart[pl.ds(base, span)] = wpart[pl.ds(base, span)] + out if add else out

    pairs, quads, far = span // 2, span // 4, span // 4

    def half1(j, p):
        at = pl.ds(unit_of(j, p)[1] // 2, pairs)
        k = j * owned + p
        return remote(send1.at[at], recv1.at[at], ws.at[0, k], wr.at[0, k], (mate0, tp))

    half = chans // 2

    def cols(h):
        return pl.ds(h * half, half)

    def half2(j, p, h):
        at = (pl.ds(unit_of(j, p)[1] // 4, quads), slice(None), cols(h))
        k = j * owned + p
        return remote(send2.at[at], recv2.at[at], ws.at[1 + h, k], wr.at[1 + h, k], (mate1, tp))

    def start1(j, p):
        first = unit_of(j, p)[1] // 2

        def cast(i):
            send1[first + i] = wpart[2 * (first + i) + 1 - b0].astype(BF16)

        loop(0, pairs, cast)
        half1(j, p).start()

    def start2(j, p):
        first = unit_of(j, p)[1] // 4
        half1(j, p).wait_recv()
        for h in range(2):
            def cast(i, h=h):
                other = 2 * (first + i) + 1 - b1
                send2[first + i, :, cols(h)] = (
                    wpart[2 * other + b0, :, cols(h)] + recv1[other, :, cols(h)].astype(F32)).astype(BF16)

            loop(0, quads, cast)
            half2(j, p, h).start()

        def keep(i):
            mine = 2 * (first + i) + b1
            wpart[2 * mine + b0] = wpart[2 * mine + b0] + recv1[mine].astype(F32)

        loop(0, quads, keep)

    def total2(z, h):
        return wpart[4 * z + 2 * b1 + b0, :, cols(h)] + recv2[z, :, cols(h)].astype(F32)

    def final_copy(slot, h):
        at = (slot, slice(None), cols(h))
        return remote(send3.at[at], recv3.at[at], ws3.at[h, slot], wr3.at[h, slot],
                      (lax.rem(sp + 4 * (slot + 1), n), tp))

    def start3(j, p, h):
        half2(j, p, h).wait_recv()
        first = unit_of(j, p)[1] // 4

        def one(i):
            z = first + i
            d = lax.rem(z + group - zz, group)

            @pl.when(d != 0)
            def _():
                send3[d - 1, :, cols(h)] = total2(z, h).astype(BF16)
                final_copy(d - 1, h).start()

        loop(0, far, one)

    def weight_rows(j, lane):
        return pl.ds(pl.multiple_of(owner(j) * chans + lane, UNIT), UNIT)

    def own_ng(r):
        at = pl.ds(pl.multiple_of(r * nstep, nstep), nstep)
        ngacc[at, :] = jnp.dot(grad[at, :], weight[pl.ds(pl.multiple_of(owner(0) * chans, UNIT), chans), :],
                               preferred_element_type=F32)

    def unit_ng(p):
        def add(r):
            at = pl.ds(pl.multiple_of(r * nstep, nstep), nstep)
            lane = unit_lane_from(p)
            j = p // owned + 1
            ngacc[at, :] += jnp.dot(others[j - 1, at, pl.ds(lane, UNIT)], weight[weight_rows(j, lane), :],
                                    preferred_element_type=F32)

        loop(0, rows // nstep, add)

    def middle(r):
        at = pl.ds(pl.multiple_of(r * CHUNK, CHUNK), CHUNK)
        ng = ngacc[at, :] + jnp.dot(others[peers - 2, at, :], weight[pl.ds(pl.multiple_of(owner(peers - 1) * chans, UNIT), chans), :],
                                    preferred_element_type=F32)
        act_to_conv(ng, pl.multiple_of(r * CHUNK + EDGE, 8), CHUNK, True, unit, inv, slope, gain, dconv, gain_part, apart)

    def taps_chunks(*rs, flat=False):
        def tile(c):
            for i, r in enumerate(rs):
                for tau in range(TAU):
                    low = r * CHUNK + (EDGE + tau)
                    dpack[c, i * TAU + tau] = spread(dconv, c, low, low + TAU * (SEG // 2), TAU)
            for k0 in range(0, kw, 4):
                ks = range(k0, min(k0 + 4, kw))
                pairs_ = [[((lambda r=r, j=tau + k: shifted[c, r, j]), (lambda i=i, tau=tau: dpack[c, i * TAU + tau]))
                           for i, r in enumerate(rs) for tau in range(TAU)] for k in ks]
                for k, total in zip(ks, products(pairs_)):
                    tacc[c, k] += total[:SEG // 2] + total[SEG // 2:]

        if flat:
            for c in range(tiles):
                tile(c)
        else:
            loop(0, tiles, tile)

    def finalize(r):
        gather(units - 1, r).wait_recv()
        middle(r)

    def finalize_two(i):
        finalize(2 * i)
        finalize(2 * i + 1)
        taps_chunks(2 * i, 2 * i + 1)

    def fold_taps(c):
        for k in range(kw):
            sums[c, pl.ds(k, 1), :] = jnp.sum(tacc[c, k], axis=0, keepdims=True)
        sums[c, pl.ds(kw, 1), :] = jnp.sum(gain_part[:, lanes(c)], axis=0, keepdims=True)

    def edge_conv():
        for side, at in ((0, 0), (1, rows + EDGE)):
            @pl.when(arrives[side])
            def _(side=side, at=at):
                for copy in ohalos[side]:
                    copy.wait_recv()
                ng = sum(jnp.dot(ohalo[side, j], weight[pl.ds(pl.multiple_of(owner(j) * chans, UNIT), chans), :],
                                 preferred_element_type=F32) for j in range(peers))
                act_to_conv(ng, at, EDGE, False, unit, inv, slope, gain, dconv, gain_part, apart)

            @pl.when(jnp.logical_not(arrives[side]))
            def _(at=at):
                for c in range(tiles):
                    dconv[c, pl.ds(at, EDGE), :] = jnp.zeros((EDGE, LANE), F32)

    def backward(r):
        def tile(c):
            base = r * CHUNK
            for j in range(TAU + kw - 1):
                low = base + (EDGE - kw // 2 + j)
                dshift[j] = spread(dconv, c, low, low + TAU * (SEG // 2), TAU)

            def put(tau, total):
                for h in range(2):
                    grow[c, pl.ds(tau + h * TAU * (SEG // 2), SEG // 2, stride=TAU), :] = (
                        total[h * (SEG // 2):(h + 1) * (SEG // 2)])

            conv_block(kw, lambda j: dshift[j], tapb, c, TAU, True, put)
            at = pl.ds(pl.multiple_of(base, CHUNK), CHUNK)
            s = sigmoid(gate[at, lanes(c)].astype(F32))
            v = value[at, lanes(c)].astype(F32)
            out = grow[c] * s
            vgrad[at, lanes(c)] = out.astype(BF16)
            ggrad[at, lanes(c)] = (out * v * (1.0 - s)).astype(BF16)

        loop(0, tiles, tile)

    part = (kw + 1) // 2
    collects = b0 == 1

    def collector(q):
        return sp - quarter + 2 * q + 1

    def gather_sums(q, sender):
        return remote(asend.at[q], arecv.at[sender], as_.at[0, q], ar.at[0, sender], (collector(q), tp))

    def other(d):
        return lax.rem(quarter + d, 4)

    def share(d):
        return remote(atotal.at[b1], atotal.at[b1], as_.at[1, d - 1], ar.at[1, b1], (plane(d), tp))

    def spread_sums(d):
        return remote(zsend, zrecv.at[zz], as3.at[d - 1], ar3.at[d - 1], (zmate(d), tp))

    def shared(q):
        return remote(atotal.at[q], atotal.at[q], as_.at[1, 0], ar.at[1, q], (plane(1), tp))

    loads[2].wait()
    for p in range(owned):
        weight_part(0, p, 0, rows, False)
        start1(0, p)
    loads[5].wait()
    loop(0, rows // nstep, own_ng)
    for p in range(owned):
        start2(0, p)
    for p in range(units - 1):
        for r in range(chunks):
            gather(p, r).wait_recv()
        weight_part(p // owned + 1, p % owned, 0, rows, False)
        start1(p // owned + 1, p % owned)
        if p < units - owned:
            unit_ng(p)
    for p in range(owned):
        for h in range(2):
            start3(0, p, h)
    for p in range(units - 1):
        start2(p // owned + 1, p % owned)
    lj, lp = peers - 1, owned - 1
    loop(0, 2, finalize_two)
    for p in range(units - 1):
        for h in range(2):
            start3(p // owned + 1, p % owned, h)
    loop(2, chunks // 2 - 2, finalize_two)
    gather(units - 1, chunks - 4).wait_recv()
    pl.when(b0 == 1)(start_held)
    middle(chunks - 4)
    finalize(chunks - 3)
    taps_chunks(chunks - 4, chunks - 3)
    weight_part(lj, lp, 0, rows - 2 * CHUNK, False)
    finalize(chunks - 2)
    taps_chunks(chunks - 2)
    gather(units - 1, chunks - 1).wait_recv()
    middle(chunks - 1)
    taps_chunks(chunks - 1, flat=True)
    loop(0, tiles, fold_taps)
    for q in range(2):
        asend[q] = sums[:, q * part:(q + 1) * part, :].astype(BF16)

        @pl.when(quarter != 2 * q + 1)
        def _(q=q):
            gather_sums(q, quarter).start()

    start_halos(ohalos)
    weight_part(lj, lp, rows - 2 * CHUNK, 2 * CHUNK, True)
    start1(lj, lp)
    loop(1, 3, backward)
    start2(lj, lp)
    backward(3)

    @pl.when(collects)
    def _():
        for d in range(1, 4):
            gather_sums(0, other(d)).wait_recv()
        mine = sums[:, pl.ds(pl.multiple_of(b1 * part, part), part), :]
        for d in range(1, 4):
            mine += arecv[other(d)].astype(F32)
        zsend[...] = mine.astype(BF16)
        for d in range(1, group):
            spread_sums(d).start()

    loop(4, chunks - 1, backward)
    start3(lj, lp, 0)
    start3(lj, lp, 1)

    @pl.when(collects)
    def _():
        zrecv[zz] = zsend[...]
        for d in range(1, group):
            peer = lax.rem(zz + group - d, group)
            remote(zsend, zrecv.at[peer], as3.at[d - 1], ar3.at[d - 1], (zmate(d), tp)).wait_recv()
        total = zrecv[0].astype(F32)
        for z in range(1, group):
            total += zrecv[z].astype(F32)
        atotal[b1] = total
        for d in (1, 3, 2):
            share(d).start()

    edge_conv()
    loop(0, 2, lambda i: backward(i * (chunks - 1)))
    for h in range(2):
        final = total2(zz, h)
        for d in range(1, group):
            final_copy(d - 1, h).wait_recv()
            final += recv3[d - 1, :, cols(h)].astype(F32)
        wout[:, cols(h)] = final
    for q in range(2):
        @pl.when(quarter != 2 * q + 1)
        def _(q=q):
            shared(q).wait_recv()

    for c in range(tiles):
        tot = jnp.concatenate([atotal[q, c] for q in range(2)], axis=0)
        taps_out[:, c * LANE:(c + 1) * LANE] = tot[:kw]
        gain_out[:, c * LANE:(c + 1) * LANE] = tot[kw:]
    for q in range(2):
        @pl.when(quarter != 2 * q + 1)
        def _(q=q):
            gather_sums(q, quarter).wait_send()

    @pl.when(collects)
    def _():
        for d in range(1, 4):
            share(d).wait_send()
        for d in range(1, group):
            spread_sums(d).wait_send()

    for side in range(2):
        @pl.when(sends[side])
        def _(side=side):
            for copy in halos[side] + ohalos[side]:
                copy.wait_send()
    for p in range(units):
        for r in range(chunks):
            gather(p, r).wait_send()
    for j in range(peers):
        for p in range(owned):
            half1(j, p).wait_send()
            for h in range(2):
                half2(j, p, h).wait_send()
    for d in range(1, group):
        for h in range(2):
            final_copy(d - 1, h).wait_send()


def finish_kernel(parts, *refs):
    count = len(parts)
    sources, targets = refs[:count], refs[count:]

    def move(osem):
        outgoing = []
        for src, dst, pieces in zip(sources, targets, parts):
            size = src.shape[0] // pieces
            for p in range(pieces):
                at = pl.ds(p * size, size)
                outgoing.append(pltpu.make_async_copy(src.at[at], dst.at[at], osem.at[len(outgoing)]))
        for copy in outgoing:
            copy.start()
        for copy in outgoing:
            copy.wait()

    pl.run_scoped(move, pltpu.SemaphoreType.DMA((sum(parts),)))


def finish(*arrays):
    parts = [4 if a.shape[0] % 128 == 0 else 1 for a in arrays]
    return pl.pallas_call(
        functools.partial(finish_kernel, parts),
        out_shape=[jax.ShapeDtypeStruct(a.shape, a.dtype) for a in arrays],
        in_specs=[pl.BlockSpec(memory_space=pltpu.VMEM)] * len(arrays),
        out_specs=[pl.BlockSpec(memory_space=pl.ANY)] * len(arrays),
    )(*[pltpu.with_memory_space_constraint(a, pltpu.VMEM) for a in arrays])


def per_device(value, gate, conv_taps, norm_gain, point_weight, out_grad):
    rows, chans = value.shape
    kw = conv_taps.shape[0]
    tiles = chans // LANE
    n, peers = lax.axis_size("sp"), lax.axis_size("tp")
    extent = rows + WIDE
    full = point_weight.shape[0]
    per = full // n
    group = n // 4
    chunks = rows // CHUNK
    owned = chans // UNIT
    units = (peers - 1) * owned
    gain = norm_gain.reshape(1, chans)
    args = (value, gate, conv_taps, gain, point_weight, out_grad)
    piece = (tiles, (kw + 1) // 2, LANE)
    vmem, dma = pltpu.VMEM, pltpu.SemaphoreType.DMA
    block = (SEG, LANE)
    outs = [((rows, chans), BF16), ((rows, chans), BF16), ((kw, chans), F32), ((1, chans), F32), ((per, chans), F32)]
    semaphores = [
            dma((6,)),
            dma((2, 2)), dma((2, 2)), dma((2, peers)), dma((2, peers)),
            dma((units, chunks)), dma((units, chunks)),
            dma((3, peers * owned)), dma((3, peers * owned)), dma((2, group - 1)), dma((2, group - 1)),
            dma((2, 3)), dma((2, 4)), dma((group - 1,)), dma((group - 1,)),
    ]

    def scoped_kernel(*refs):
        pl.run_scoped(lambda *held: whole_kernel(n, peers, *refs, *held), *semaphores)

    vgrad, ggrad, taps_grad, gain_grad, wgrad = pl.pallas_call(
        scoped_kernel,
        out_shape=[vmem(s, d) for s, d in outs],
        in_specs=[pl.BlockSpec(memory_space=pl.ANY)] * 6,
        out_specs=[pl.BlockSpec(memory_space=vmem)] * len(outs),
        scratch_shapes=[
            vmem((rows, chans), BF16), vmem((rows, chans), BF16), vmem((full, chans), BF16), vmem((rows, chans), BF16),
            vmem((kw, chans), BF16), vmem((1, chans), F32),
            vmem((tiles, kw, LANE), F32),
            vmem((tiles, kw) + block, BF16),
            vmem((tiles, kw, 8, LANE), F32),
            vmem((tiles, rows + 4 * EDGE, LANE), F32),
            vmem((tiles, chunks, TAU + kw - 1) + block, BF16),
            vmem((kw + 1,) + block, BF16),
            vmem((tiles, extent, LANE), F32),
            vmem((tiles, extent, LANE), F32),
            vmem((tiles, extent, LANE), F32),
            vmem((rows, chans), BF16),
            vmem((tiles, extent, LANE), F32),
            vmem((TAU + kw - 1,) + block, BF16),
            vmem((tiles, 2 * TAU) + block, BF16),
            vmem((tiles, CHUNK, LANE), F32),
            vmem((rows, chans), F32),
            vmem((8, chans), F32),
            vmem((n, per, chans), F32),
            vmem((tiles, kw + 1, LANE), F32),
            vmem((2, 2, WIDE, chans), BF16),
            vmem((2, peers, EDGE, chans), BF16),
            vmem((peers - 1, rows, chans), BF16),
            vmem((n // 2, per, chans), BF16),
            vmem((n // 2, per, chans), BF16),
            vmem((n // 4, per, chans), BF16),
            vmem((n // 4, per, chans), BF16),
            vmem((group - 1, per, chans), BF16),
            vmem((group - 1, per, chans), BF16),
            vmem((2,) + piece, BF16),
            vmem((4,) + piece, BF16),
            vmem((2,) + piece, F32),
            vmem(piece, BF16),
            vmem((group,) + piece, BF16),
        ],
        compiler_params=pltpu.CompilerParams(
            collective_id=0, has_side_effects=True, vmem_limit_bytes=52 * 1024 * 1024),
    )(*args)
    vgrad, ggrad, taps_grad, gain_grad, wgrad = finish(vgrad, ggrad, taps_grad, gain_grad, wgrad)
    return vgrad, ggrad, taps_grad, gain_grad.reshape(chans), wgrad


def solution(mesh):
    return jax.shard_map(
        per_device,
        mesh=mesh,
        in_specs=(P("sp", "tp"), P("sp", "tp"), P(None, "tp"), P("tp"), P(None, "tp"), P("sp", "tp")),
        out_specs=(P("sp", "tp"), P("sp", "tp"), P(None, "tp"), P("tp"), P("sp", "tp")),
        check_vma=False,
    )
```
